256 devices in a mesh: sp: 16 (over y, x), tp: 16 (over z, core).
Axes of the slice: x: 4, y: 4, z: 8, core: 2. Of those that a mesh axis runs over, the one named last changes fastest.
Arguments:
- query_a: bfloat16 [4096, 16, 256], P('sp', 'tp'), may hold values from -5.5 to 5.5
- key_a: bfloat16 [4096, 16, 256], P('sp', 'tp'), may hold values from -5.5 to 5.5
- value_a: bfloat16 [4096, 16, 256], P('sp', 'tp'), may hold values from -6 to 6
- query_b: bfloat16 [4096, 16, 128], P('sp', 'tp'), may hold values from -5.5 to 5.5
- key_b: bfloat16 [4096, 16, 128], P('sp', 'tp'), may hold values from -5.5 to 5.5
- value_b: bfloat16 [4096, 16, 128], P('sp', 'tp'), may hold values from -6 to 6
- lambdas: float32 [2, 16], P(None, 'tp'), may hold values from 0.3 to 0.8
- gain_a: float32 [256], replicated, may hold values from 0.1 to 1.9
- gain_b: float32 [128], replicated, may hold values from 0.1 to 1.9
- out_a: bfloat16 [4096, 4096], P('tp'), may hold values from -0.078125 to 0.078125
- out_b: bfloat16 [2048, 4096], P('tp'), may hold values from -0.078125 to 0.078125
- residual: bfloat16 [4096, 4096], P(('sp', 'tp')), may hold values from -6 to 6
- norm_gain: float32 [4096], replicated, may hold values from 0.1 to 1.9
- route_ids: int32 [4096, 2], P(('sp', 'tp')), may hold values from 0 to 31, all different within a row; in each aligned block of 16 rows (0 to 15, 16 to 31, ...) at most 2 rows name the same one
- route_weights: float32 [4096, 2], P(('sp', 'tp')), may hold values from 0.1 to 0.9
- w_gate: bfloat16 [32, 4096, 2048], P('sp', None, 'tp'), may hold values from -0.28125 to 0.28125
- w_up: bfloat16 [32, 4096, 2048], P('sp', None, 'tp'), may hold values from -0.28125 to 0.28125
- w_down: bfloat16 [32, 2048, 4096], P('sp', 'tp'), may hold values from -0.01977539 to 0.01977539
Outputs:
- result: bfloat16 [4096, 4096], P(('sp', 'tp'))
The draws below stay inside these ranges and needn't reach their ends.
Inputs may be any that keep to these rules, and one draw needn't show every extreme that they name: `route_ids`: in the rows of one device each token names 2 different experts, no expert is named more than 2 times, a bound that some block reaches.
All inputs are finite; a program needn't handle non-finite values.
Results may differ from the reference program's by a relative error of at most 0.02.
Values may be sent and summed in bfloat16 or wider, within the bound.
No kernel may reach another device: no remote copies, remote signals or barrier semaphores. Data moves between devices by JAX's collectives and lax.ppermute only.
A program may use at most 128 MiB of HBM per device.

```python
import math
import jax
import jax.numpy as jnp
import numpy as np
from jax import lax

D = 4096
HEADS = 16
DA = 128
DB = 64
VA = 256
VB = 128
F = 2048
TOPK = 2
ROWS = 16
EXPERTS = 32
TOK_DEV = 256
SEQ = 4096
CAP = 2
N_SP = 16
N_TP = 16


def paired_maps(key, salt, width):
    base = jax.random.fold_in(key, salt)
    key_query, key_keys = jax.random.split(base, 2)
    shape = (SEQ, HEADS, 2 * width)
    queries = jnp.clip(1.3 * jax.random.normal(key_query, shape, jnp.float32), -5.5, 5.5)
    keys = jnp.clip(1.3 * jax.random.normal(key_keys, shape, jnp.float32), -5.5, 5.5)
    return (queries, keys)


def draw_query_a(key, part):
    return paired_maps(key, 101, DA)[0].astype(jnp.bfloat16)


def draw_key_a(key, part):
    return paired_maps(key, 101, DA)[1].astype(jnp.bfloat16)


def draw_query_b(key, part):
    return paired_maps(key, 202, DB)[0].astype(jnp.bfloat16)


def draw_key_b(key, part):
    return paired_maps(key, 202, DB)[1].astype(jnp.bfloat16)


def shard_levels(own_key, shape, cuts, least, high):
    loudness, own = 1.0, jax.random.fold_in(own_key, 6)
    for dim, blocks in cuts:
        heights = jnp.exp(jax.random.uniform(jax.random.fold_in(own, dim), (blocks,), jnp.float32, least / len(cuts), high / len(cuts)))
        loudness = loudness * jnp.repeat(heights, shape[dim] // blocks).reshape([-1 if axis == dim else 1 for axis in range(len(shape))])
    return loudness


def routed_block(rng, own, number, rows, count, top, bound, lean):
    sequence = jax.random.permutation(rng, count)
    packed, common = shares(count, rows * top, bound, lean, True), shares(count, rows * top, bound, lean, False)
    places = jnp.arange(count)

    def named(sizes, rotation):
        used = int((sizes > 0).sum())
        fixed = max(1, used // 4)
        shifted = fixed + (places - fixed + rotation * (used - fixed)) % max(1, count - fixed)
        return jnp.zeros((count,), jnp.int32).at[sequence[jnp.where(places < fixed, places, shifted)]].set(jnp.asarray(sizes, jnp.int32))

    sizes = jnp.where(number % 4 == 0, named(packed, number // 4), named(common, number - number // 4 - 1))
    mixed = jax.random.permutation(jax.random.fold_in(own, 3), count)
    donor, sink = mixed[0:count // 2 * 2:2], mixed[1:count // 2 * 2:2]
    margin = jnp.minimum(sizes[donor] - 1, bound - sizes[sink]) // 2
    margin = jnp.where((donor == sequence[0]) | (sink == sequence[0]) | (sizes[sink] == 0), 0, jnp.maximum(margin, 0))
    shifted = jax.random.randint(jax.random.fold_in(own, 4), (count // 2,), 0, 1 << 20) % (margin + 1)
    sizes = sizes.at[donor].add(-shifted).at[sink].add(shifted)
    items = jnp.searchsorted(jnp.cumsum(sizes), jnp.arange(rows * top), side="right").astype(jnp.int32)
    grid = items.reshape(top, rows).T
    grid = grid[jax.random.permutation(jax.random.fold_in(own, 1), rows)]
    rotation = jax.random.randint(jax.random.fold_in(own, 2), (rows, 1), 0, top)
    return jnp.take_along_axis(grid, (jnp.arange(top)[None, :] + rotation) % top, axis=1)


def shares(amount, total, limit, skew, full):
    loads = [(1 << 20) // math.isqrt(standing ** skew) + 1 for standing in range(1, amount + 1)]
    largest = limit if full else min(limit, max(-(-total // amount), total * loads[0] // sum(loads)))
    least = 1 if total - largest >= amount - 1 else 0
    given, spare = [largest] + [least] * (amount - 1), total - largest - least * (amount - 1)
    while spare > 0:
        candidates = [i for i in range(1, amount) if given[i] < largest] or [i for i in range(1, amount) if given[i] < limit]
        pool, budget = sum([loads[i] for i in candidates]), spare
        for i in candidates:
            more = min(limit - given[i], max(1, budget * loads[i] // pool), spare)
            given[i] = given[i] + more
            spare = spare - more
    return np.array(given)


def bell_draw(stream_key, dims, scale, most, cuts=(), kind=jnp.bfloat16):
    entries = scale * jax.random.normal(stream_key, dims, jnp.float32)
    if cuts:
        entries = entries * shard_levels(stream_key, dims, cuts, -0.22, 0.18)
    return jnp.clip(entries, -most, most).astype(kind)


def setup_inputs(seed: int = 0) -> dict:
    arg_keys = jax.random.split(jax.random.key(seed), 19)
    query_a = draw_query_a(jax.random.fold_in(arg_keys[18], 71), 0)
    key_a = draw_key_a(jax.random.fold_in(arg_keys[18], 71), 0)
    value_a = bell_draw(arg_keys[2], (SEQ, HEADS, VA), 1.0, 6.0, ((0, 16), (1, 16)))
    query_b = draw_query_b(jax.random.fold_in(arg_keys[18], 71), 0)
    key_b = draw_key_b(jax.random.fold_in(arg_keys[18], 71), 0)
    value_b = bell_draw(arg_keys[5], (SEQ, HEADS, VB), 1.0, 6.0, ((0, 16), (1, 16)))
    lambdas = jnp.clip(0.3 + 0.5 * jax.random.uniform(arg_keys[6], (2, HEADS), jnp.float32) ** shard_levels(arg_keys[6], (2, HEADS), ((1, 16),), -0.2, 0.2), 0.3, 0.8)
    gain_a = jnp.clip(1.0 + 0.18 * jax.random.normal(arg_keys[7], (VA,), jnp.float32), 0.1, 1.9)
    gain_b = jnp.clip(1.0 + 0.18 * jax.random.normal(arg_keys[8], (VB,), jnp.float32), 0.1, 1.9)
    out_a = bell_draw(arg_keys[9], (HEADS * VA, D), (HEADS * (VA + VB)) ** -0.5, 0.078125, ((0, 16),))
    out_b = bell_draw(arg_keys[10], (HEADS * VB, D), (HEADS * (VA + VB)) ** -0.5, 0.078125, ((0, 16),))
    residual = bell_draw(arg_keys[11], (SEQ, D), 1.0, 6.0, ((0, 256),))
    norm_gain = jnp.clip(1.0 + 0.18 * jax.random.normal(arg_keys[12], (D,), jnp.float32), 0.1, 1.9)
    route_ids_keys = jax.random.split(jax.random.fold_in(arg_keys[13], 1), SEQ // ROWS)
    route_ids_turns = jax.random.permutation(jax.random.fold_in(arg_keys[13], 3), SEQ // ROWS)
    route_ids = jax.vmap(lambda own, number: routed_block(jax.random.fold_in(arg_keys[13], 2), own, number, ROWS, EXPERTS, TOPK, CAP, 2))(route_ids_keys, route_ids_turns).reshape((SEQ, TOPK))
    route_weights = jnp.clip(0.1 + 0.79999997 * jax.random.uniform(arg_keys[14], (SEQ, TOPK), jnp.float32) ** shard_levels(arg_keys[14], (SEQ, TOPK), ((0, 256),), -0.2, 0.2), 0.1, 0.9)
    w_gate = bell_draw(arg_keys[15], (EXPERTS, D, F), (3.0 / D ** 0.5), 0.28125, ((0, 16), (2, 16)))
    w_up = bell_draw(arg_keys[16], (EXPERTS, D, F), (3.0 / D ** 0.5), 0.28125, ((0, 16), (2, 16)))
    w_down = bell_draw(arg_keys[17], (EXPERTS, F, D), (0.15 / F ** 0.5), 0.01977539, ((0, 16), (1, 16)))
    return dict(query_a=query_a, key_a=key_a, value_a=value_a, query_b=query_b, key_b=key_b, value_b=value_b, lambdas=lambdas, gain_a=gain_a, gain_b=gain_b, out_a=out_a, out_b=out_b, residual=residual, norm_gain=norm_gain, route_ids=route_ids, route_weights=route_weights, w_gate=w_gate, w_up=w_up, w_down=w_down)


EPSILON = 1e-06
LIMIT = 7.0
SLOPE = 1.702

def head_output(query_head, key_head, value_head, lambda_head, gain, width):
    scaling = width ** (-0.5)

    def block(query_block):
        heard = []
        for which in range(2):
            query_part = query_block[:, which * width:(which + 1) * width]
            key_part = key_head[:, which * width:(which + 1) * width]
            scores = jnp.dot(query_part, key_part.T, preferred_element_type=jnp.float32) * scaling
            highest = lax.optimization_barrier(jnp.max(scores, axis=1, keepdims=True))
            expo = jnp.exp(scores - highest)
            totals = lax.optimization_barrier(jnp.sum(expo, axis=1, keepdims=True))
            summed = jnp.dot(expo.astype(jnp.bfloat16), value_head, preferred_element_type=jnp.float32)
            heard.append(summed / totals)
        differ = heard[0] - lambda_head * heard[1]
        scaled = lax.rsqrt(lax.optimization_barrier(jnp.mean(differ * differ, axis=1, keepdims=True)) + EPSILON)
        return (differ * scaled * gain).astype(jnp.bfloat16)
    blocks = query_head.reshape(SEQ // TOK_DEV, TOK_DEV, 2 * width)
    return lax.map(block, blocks).reshape(SEQ, -1)

def group_output(queries, keys, values, lambda_row, gain, width):

    def one_head(items):
        return head_output(items[0], items[1], items[2], items[3], gain, width)
    heads = lax.map(one_head, (jnp.swapaxes(queries, 0, 1), jnp.swapaxes(keys, 0, 1), jnp.swapaxes(values, 0, 1), lambda_row))
    return jnp.swapaxes(heads, 0, 1).reshape(SEQ, -1)

def reference(query_a, key_a, value_a, query_b, key_b, value_b, lambdas, gain_a, gain_b, out_a, out_b, residual, norm_gain, route_ids, route_weights, w_gate, w_up, w_down):
    attended_a = group_output(query_a, key_a, value_a, lambdas[0], gain_a, DA)
    attended_b = group_output(query_b, key_b, value_b, lambdas[1], gain_b, DB)
    projected = jnp.dot(attended_a, out_a, preferred_element_type=jnp.float32) + jnp.dot(attended_b, out_b, preferred_element_type=jnp.float32)
    mixed = (residual.astype(jnp.float32) + projected).astype(jnp.bfloat16)
    widened = mixed.astype(jnp.float32)
    normed = (widened * lax.rsqrt(lax.optimization_barrier(jnp.mean(widened * widened, axis=1, keepdims=True)) + EPSILON) * norm_gain).astype(jnp.bfloat16)
    hidden_part = F // N_TP
    most_load = N_SP * N_TP * CAP

    def expert_step(running, expert):
        chosen = route_ids == expert
        weight = lax.optimization_barrier(jnp.sum(jnp.where(chosen, route_weights, jnp.float32(0.0)), axis=1))
        marked = jnp.any(chosen, axis=1)
        picked = jnp.nonzero(marked, size=most_load, fill_value=0)[0].astype(jnp.int32)
        counted = jnp.sum(marked.astype(jnp.int32))
        valid = jnp.arange(most_load, dtype=jnp.int32) < counted
        rows = normed[picked]
        gate = jnp.dot(rows, w_gate[expert], preferred_element_type=jnp.float32)
        upward = jnp.dot(rows, w_up[expert], preferred_element_type=jnp.float32)
        clamped = jnp.minimum(gate, LIMIT)
        active = (clamped * jax.nn.sigmoid(SLOPE * clamped) * (jnp.clip(upward, -LIMIT, LIMIT) + 1.0)).astype(jnp.bfloat16)
        blocks = active.astype(jnp.float32).reshape(most_load, N_TP, hidden_part)
        down = w_down[expert].astype(jnp.float32).reshape(N_TP, hidden_part, D)
        partial_value = jnp.einsum('rjf,jfd->jrd', blocks, down).astype(jnp.bfloat16)
        partial_value = lax.optimization_barrier(partial_value)
        expert_out = lax.optimization_barrier(jnp.sum(partial_value.astype(jnp.float32), axis=0)).astype(jnp.bfloat16)
        expert_out = lax.optimization_barrier(expert_out)
        scale_rows = jnp.where(valid, weight[picked], jnp.float32(0.0))
        running = running.at[picked].add(scale_rows[:, None] * expert_out.astype(jnp.float32))
        return (running, None)
    combined, _ = lax.scan(expert_step, jnp.zeros((SEQ, D), jnp.float32), jnp.arange(EXPERTS, dtype=jnp.int32))
    return (widened + combined).astype(jnp.bfloat16)
```

```python
import functools

import jax
import jax.numpy as jnp
from jax import lax
from jax.experimental import pallas as pl
from jax.experimental.pallas import tpu as pltpu
from jax.sharding import Mesh
from jax.sharding import PartitionSpec as P


TP = ("z", "c")
SP = ("y", "x")
ALL = ("y", "x", "z", "c")

EPSILON = 1e-06
LIMIT = 7.0
SLOPE = 1.702
LOG2E = 1.4426950408889634

N4 = 4
NZ = 8
TOK = 256
KEYS = N4 * TOK
CHUNK = 128
STAT = 16
DA = 128
DB = 64
VA = 256
VB = 128
f32 = jnp.float32
bf16 = jnp.bfloat16


def shifted(array, axis, count, by):
    return lax.ppermute(array, axis, [(i, (i + by) % count) for i in range(count)])


def one_group(q_scr, k_scr, v_scr, o_scr, block, row, width, packed):
    rows = pl.ds(pl.multiple_of(row * CHUNK, CHUNK), CHUNK)
    q = q_scr[block, rows, :]
    value_width = v_scr.shape[1]
    scaling = width ** (-0.5) * LOG2E
    lane = lax.broadcasted_iota(jnp.int32, (CHUNK, 128), 1)
    stats = jnp.zeros((CHUNK, 128), f32)
    for which in range(2):
        if packed:
            mine = lax.broadcasted_iota(jnp.int32, q.shape, 1) // width == which
            part = jnp.where(mine, q, jnp.zeros_like(q))
            keys = k_scr[...]
        else:
            part = q[:, which * width : (which + 1) * width]
            keys = k_scr[:, which * width : (which + 1) * width]
        scores = (
            lax.dot_general(part, keys, (((1,), (1,)), ((), ())), preferred_element_type=f32)
            * scaling
        )
        highest = jnp.max(scores, axis=1, keepdims=True).astype(bf16).astype(f32)
        expo = jnp.exp2(scores - highest)
        total = jnp.sum(expo, axis=1, keepdims=True)
        carried = jnp.dot(expo.astype(bf16), v_scr[...], preferred_element_type=f32)
        o_scr[block, rows, which * value_width : (which + 1) * value_width] = carried.astype(bf16)
        coarse = total.astype(bf16).astype(f32)
        for at, stat in enumerate((highest, coarse, total - coarse)):
            stats = jnp.where(lane == 3 * which + at, stat, stats)
    o_scr[block, TOK : TOK + STAT, rows] = stats.T[:STAT, :].astype(bf16)


def partial_kernel(blocks, *refs):
    xs, ys = refs[:4], refs[4:8]
    count = len(blocks)
    outs_a, outs_b = refs[8 : 8 + count], refs[8 + count : 8 + 2 * count]
    qa, ka, va, oa, qb, kb, vb, ob = refs[8 + 2 * count :]
    for i in range(4):
        rows = slice(i * TOK, (i + 1) * TOK)
        ka[rows, :] = xs[i][:, : 2 * DA]
        va[rows, :] = xs[i][:, 2 * DA : 2 * DA + VA]
        kb[rows, :] = ys[i][:, : 2 * DB]
        vb[rows, :] = ys[i][:, 2 * DB : 2 * DB + VB]
    for at, i in enumerate(blocks):
        qa[at] = ys[i][:, 2 * DB + VB :]
        qb[at] = xs[i][:, 2 * DA + VA :]
        oa[at, TOK:, :] = jnp.zeros((STAT, 2 * VA), bf16)
        ob[at, TOK:, :] = jnp.zeros((STAT, 2 * VB), bf16)
    per = TOK // CHUNK

    def step(n, carry):
        block, row = n // per, n % per
        one_group(qa, ka, va, oa, block, row, DA, False)
        one_group(qb, kb, vb, ob, block, row, DB, True)
        return carry

    lax.fori_loop(0, count * per, step, 0)
    for at in range(count):
        outs_a[at][...] = oa[at]
        outs_b[at][...] = ob[at]


def partial_attention(xs, ys, blocks):
    count = len(blocks)
    vmem = pl.BlockSpec(memory_space=pltpu.VMEM)
    shapes = [jax.ShapeDtypeStruct((TOK + STAT, 2 * VA), bf16)] * count
    shapes += [jax.ShapeDtypeStruct((TOK + STAT, 2 * VB), bf16)] * count
    outs = pl.pallas_call(
        functools.partial(partial_kernel, blocks),
        out_shape=shapes,
        in_specs=[vmem] * 8,
        out_specs=[vmem] * (2 * count),
        scratch_shapes=[
            pltpu.VMEM((count, TOK, 2 * DA), bf16),
            pltpu.VMEM((KEYS, 2 * DA), bf16),
            pltpu.VMEM((KEYS, VA), bf16),
            pltpu.VMEM((count, TOK + STAT, 2 * VA), bf16),
            pltpu.VMEM((count, TOK, 2 * DB), bf16),
            pltpu.VMEM((KEYS, 2 * DB), bf16),
            pltpu.VMEM((KEYS, VB), bf16),
            pltpu.VMEM((count, TOK + STAT, 2 * VB), bf16),
        ],
        cost_estimate=pl.CostEstimate(
            flops=count * 604_000_000, bytes_accessed=4_000_000, transcendentals=count * 1_048_576
        ),
    )(*xs, *ys)
    return outs[:count], outs[count:]


def merge_group(parts, stat_scr, rows, value_width, weight, gain):
    lanes = stat_scr[rows, :]
    column = lambda part, at: lanes[:, STAT * part + at : STAT * part + at + 1]
    heard = []
    for which in range(2):
        maxima = [column(i, 3 * which) for i in range(4)]
        highest = jnp.maximum(jnp.maximum(maxima[0], maxima[1]), jnp.maximum(maxima[2], maxima[3]))
        total, summed = 0.0, 0.0
        for i in range(4):
            factor = jnp.exp2(maxima[i] - highest)
            total = total + factor * (column(i, 3 * which + 1) + column(i, 3 * which + 2))
            values = parts[i][rows, which * value_width : (which + 1) * value_width]
            summed = summed + factor * values.astype(f32)
        heard.append(summed / total)
    differ = heard[0] - weight * heard[1]
    scaled = lax.rsqrt(jnp.mean(differ * differ, axis=1, keepdims=True) + EPSILON)
    return (differ * scaled * gain).astype(bf16)


def merge_kernel(core, lam, gain_a, gain_b, *refs):
    pa, pb = refs[:4], refs[4:8]
    away, mine, sa, sb, att = refs[-5:]
    for parts, scr in ((pa, sa), (pb, sb)):
        rows = [p[TOK:, :TOK].astype(f32) for p in parts]
        rows.append(jnp.zeros((128 - 4 * STAT, TOK), f32))
        scr[...] = jnp.concatenate(rows, axis=0).T

    def step(n, carry):
        rows = pl.ds(pl.multiple_of(n * 64, 64), 64)
        att[rows, :VA] = merge_group(pa, sa, rows, VA, lam[0], gain_a[...])
        att[rows, VA:] = merge_group(pb, sb, rows, VB, lam[1], gain_b[...])
        return carry

    lax.fori_loop(0, TOK // 64, step, 0)
    half = TOK // 2
    me = core[0]
    away[...] = att[pl.ds(pl.multiple_of((1 - me) * half, half), half), :]
    mine[...] = att[pl.ds(pl.multiple_of(me * half, half), half), :]


def merged(parts_a, parts_b, lam, gain_a, gain_b, core, first):
    smem = pl.BlockSpec(memory_space=pltpu.SMEM)
    vmem = pl.BlockSpec(memory_space=pltpu.VMEM)
    out = jax.ShapeDtypeStruct((TOK // 2, VA + VB), bf16)
    return pl.pallas_call(
        merge_kernel,
        out_shape=[out, out],
        in_specs=[smem, smem] + [vmem] * 10 + [pl.BlockSpec(memory_space=pl.ANY)] * len(first),
        out_specs=[vmem, vmem],
        scratch_shapes=[
            pltpu.VMEM((TOK, 128), f32),
            pltpu.VMEM((TOK, 128), f32),
            pltpu.VMEM((TOK, VA + VB), bf16),
        ],
        cost_estimate=pl.CostEstimate(
            flops=800_000_000, bytes_accessed=2_000_000, transcendentals=20_000
        ),
        name="merge_parts",
    )(
        core.reshape(1),
        lam,
        gain_a.reshape(1, -1),
        gain_b.reshape(1, -1),
        *parts_a,
        *parts_b,
        *first,
    )


def project_kernel(mine, joined, wa, wb, xa, xb, out):
    total = jnp.dot(mine[:, :VA], wa[...], preferred_element_type=f32)
    total += jnp.dot(joined[:, :VA], xa[...], preferred_element_type=f32)
    total += jnp.dot(mine[:, VA:], wb[...], preferred_element_type=f32)
    total += jnp.dot(joined[:, VA:], xb[...], preferred_element_type=f32)
    out[...] = total


def project(mine, joined, wa, wb, xa, xb):
    width, tile = wa.shape[1], 1024
    whole = pl.BlockSpec(mine.shape, lambda i: (0, 0))
    deep = pl.BlockSpec((VA, tile), lambda i: (0, i))
    flat = pl.BlockSpec((VB, tile), lambda i: (0, i))
    return pl.pallas_call(
        project_kernel,
        grid=(width // tile,),
        out_shape=jax.ShapeDtypeStruct((mine.shape[0], width), f32),
        in_specs=[whole, whole, deep, flat, deep, flat],
        out_specs=pl.BlockSpec((mine.shape[0], tile), lambda i: (0, i)),
        cost_estimate=pl.CostEstimate(
            flops=3_000_000_000, bytes_accessed=8_000_000, transcendentals=0
        ),
        name="project",
    )(mine, joined, wa, wb, xa, xb)


def sum_over_z(own):
    z = lax.axis_index("z")
    pick = lambda k: lax.dynamic_index_in_dim(own, (z + k + NZ) % NZ, 0, keepdims=False)
    half = own.shape[2] // 2
    third, fourth, arrived = {}, {}, {}
    for sign in (1, -1):
        part = pick(4)[:, :half] if sign == 1 else pick(4)[:, half:]
        fourth[sign] = shifted(part.astype(bf16), "z", NZ, 2 * sign)
        third[sign] = shifted(pick(3 * sign).astype(bf16), "z", NZ, sign)
    for sign in (1, -1):
        padding = ((0, 0), (0, half)) if sign == 1 else ((0, 0), (half, 0))
        part = pick(2 * sign) + third[sign].astype(f32)
        part = part + jnp.pad(fourth[sign].astype(f32), padding)
        arrived[sign] = shifted(part.astype(bf16), "z", NZ, sign)
    for sign in (1, -1):
        part = pick(sign) + arrived[sign].astype(f32)
        arrived[sign] = shifted(part.astype(bf16), "z", NZ, sign)
    return pick(0) + arrived[1].astype(f32) + arrived[-1].astype(f32)


def attention(query_a, key_a, value_a, query_b, key_b, value_b, lambdas, gain_a, gain_b, out_a, out_b, first):
    flat = lambda a: a.reshape(TOK, -1)
    by_core = lambda a: jnp.swapaxes(a.reshape(NZ, 2, 16, -1), 0, 1).reshape(TOK, -1)
    for_x = jnp.concatenate([flat(key_a), flat(value_a), by_core(query_b)], axis=1)
    for_y = jnp.concatenate([flat(key_b), flat(value_b), by_core(query_a)], axis=1)
    order = (2, 1, 3)
    got_x = {k: shifted(for_x, "x", N4, k) for k in order}
    got_y = {k: shifted(for_y, "y", N4, k) for k in order}
    xs = [for_x] + [got_x[k] for k in (1, 2, 3)]
    ys = [for_y] + [got_y[k] for k in (1, 2, 3)]
    far_a, far_b = partial_attention(xs, ys, order)
    back = {}
    for at, k in enumerate(order):
        back[k] = (shifted(far_a[at], "y", N4, -k), shifted(far_b[at], "x", N4, -k))
    own_a, own_b = partial_attention(xs, ys, (0,))
    parts_a = [own_a[0]] + [back[k][0] for k in (1, 2, 3)]
    parts_b = [own_b[0]] + [back[k][1] for k in (1, 2, 3)]
    core = lax.axis_index("c").astype(jnp.int32)
    away, mine = merged(parts_a, parts_b, lambdas.reshape(-1), gain_a, gain_b, core, first)
    other_a, other_b = shifted(out_a, "c", 2, 1), shifted(out_b, "c", 2, 1)
    own = project(mine, shifted(away, "c", 2, 1), out_a, out_b, other_a, other_b)
    return sum_over_z(own.reshape(NZ, 16, -1))


HALVES = 2
STEP = 512


def gate_kernel(*refs):
    *pieces, weights, out, tokens, sums = refs
    rows, width = pieces[0].shape
    for at, piece in enumerate(pieces):
        row, column = at // HALVES * rows, at % HALVES * width
        tokens[row : row + rows, column : column + width] = piece[...]
    sums[...] = jnp.zeros_like(sums)

    def step(n, carry):
        part = pl.ds(pl.multiple_of(n * STEP, STEP), STEP)
        sums[...] += jnp.dot(tokens[:, part], weights[part, :], preferred_element_type=f32)
        return carry

    lax.fori_loop(0, weights.shape[0] // STEP, step, 0)
    units = out.shape[1]
    for at in range(len(pieces) // HALVES):
        here = slice(at * rows, (at + 1) * rows)
        gate = jnp.minimum(sums[here, :units], LIMIT)
        upward = jnp.clip(sums[here, units:], -LIMIT, LIMIT) + 1.0
        out[here, :] = (gate * jax.nn.sigmoid(SLOPE * gate) * upward).astype(bf16)


def gated_units(pieces, weights):
    vmem = pl.BlockSpec(memory_space=pltpu.VMEM)
    rows = len(pieces) // HALVES * pieces[0].shape[0]
    depth, both = weights.shape
    return pl.pallas_call(
        gate_kernel,
        out_shape=jax.ShapeDtypeStruct((rows, both // 2), bf16),
        in_specs=[vmem] * (len(pieces) + 1),
        out_specs=vmem,
        scratch_shapes=[pltpu.VMEM((rows, depth), bf16), pltpu.VMEM((rows, both), f32)],
        cost_estimate=pl.CostEstimate(
            flops=max(8 * rows * depth * both, 4_000_000_000),
            bytes_accessed=6_000_000,
            transcendentals=rows * 256,
        ),
    )(*pieces, weights)


def experts(block, gate_up, down):
    rows = block.shape[0]
    width = block.shape[1] // HALVES
    ring = {(0, h): block[:, h * width : (h + 1) * width] for h in range(HALVES)}
    for k in range(1, 5):
        for h in range(HALVES):
            if k < 4 or h == 0:
                ring[k, h] = shifted(ring[k - 1, h], "z", NZ, 1)
            if k < 4 or h == 1:
                ring[-k, h] = shifted(ring[1 - k, h], "z", NZ, -1)
    ring[4, 1] = ring[-4, 1]
    units = {}
    for offsets in ((0, 1, -1, 2, -2), (3, -3), (4,)):
        out = gated_units([ring[k, h] for k in offsets for h in range(HALVES)], gate_up)
        for at, k in enumerate(offsets):
            units[-k] = out[at * rows : (at + 1) * rows]
    units[4] = units[-4]

    def share(offset, h):
        return jnp.dot(
            units[offset], down[:, h * width : (h + 1) * width], preferred_element_type=f32
        )

    total = []
    carried = {}
    for k in range(4, 0, -1):
        for h in range(HALVES):
            for sign, start in ((-1, 4 - h), (1, 3 + h)):
                if k > start:
                    continue
                part = share(sign * k, h)
                if k < start:
                    part = part + carried[sign, h].astype(f32)
                carried[sign, h] = shifted(part.astype(bf16), "z", NZ, sign)
    for h in range(HALVES):
        part = share(0, h) + carried[-1, h].astype(f32) + carried[1, h].astype(f32)
        total.append(part.astype(bf16))
    return jnp.concatenate(total, axis=1)


def pack_kernel(core, gate, gate_other, upward, upward_other, down, down_other, both, lower):
    units = gate.shape[2]
    for at, ref in enumerate((gate, gate_other, upward, upward_other)):
        both[:, at * units : (at + 1) * units] = ref[0]
    for at, ref in enumerate((down, down_other)):
        lower[at * units : (at + 1) * units, :] = ref[0]


def expert_weights(w_gate, w_up, w_down, core):
    _, depth, units = w_gate.shape
    tile = 512
    deep = pl.BlockSpec((1, tile, units), lambda i, c: (c[0], i, 0))
    flat = pl.BlockSpec((1, units, tile), lambda i, c: (c[0], 0, i))
    other = lambda w: shifted(w, "c", 2, 1)
    return pl.pallas_call(
        pack_kernel,
        grid_spec=pltpu.PrefetchScalarGridSpec(
            num_scalar_prefetch=1,
            grid=(depth // tile,),
            in_specs=[deep] * 4 + [flat] * 2,
            out_specs=[
                pl.BlockSpec((tile, 4 * units), lambda i, c: (i, 0)),
                pl.BlockSpec((2 * units, tile), lambda i, c: (0, i)),
            ],
        ),
        out_shape=[
            jax.ShapeDtypeStruct((depth, 4 * units), bf16),
            jax.ShapeDtypeStruct((2 * units, depth), bf16),
        ],
        cost_estimate=pl.CostEstimate(
            flops=3_000_000_000, bytes_accessed=12_000_000, transcendentals=0
        ),
        name="pack_weights",
    )(core.reshape(1), w_gate, other(w_gate), w_up, other(w_up), w_down, other(w_down))


def slots_of(ids):
    flat = ids.reshape(-1)
    same = (flat[:, None] == flat[None, :]).astype(jnp.int32)
    place = jnp.sum(same * jnp.tril(jnp.ones_like(same), -1), axis=1)
    return (flat * 2 + place).reshape(ids.shape)


def per_device(
    query_a,
    key_a,
    value_a,
    query_b,
    key_b,
    value_b,
    lambdas,
    gain_a,
    gain_b,
    out_a,
    out_b,
    residual,
    norm_gain,
    route_ids,
    route_weights,
    w_gate,
    w_up,
    w_down,
):
    core = lax.axis_index("c").astype(jnp.int32)
    gate_up, down = expert_weights(w_gate, w_up, w_down, core)
    target = slots_of(route_ids)
    rows_here, chosen = route_ids.shape
    model_width = residual.shape[1]
    sends = 2 * N4 * N4
    slots = jnp.arange(2 * sends, dtype=jnp.int32)
    layout = jnp.any(target[None, :, :] == slots[:, None, None], axis=2).astype(bf16)
    projected = attention(
        query_a,
        key_a,
        value_a,
        query_b,
        key_b,
        value_b,
        lambdas,
        gain_a,
        gain_b,
        out_a,
        out_b,
        (layout,),
    )
    mixed = (residual.astype(f32) + projected).astype(bf16)
    widened = mixed.astype(f32)
    normed = (
        widened
        * lax.rsqrt(jnp.mean(widened * widened, axis=1, keepdims=True) + EPSILON)
        * norm_gain
    ).astype(bf16)
    leaving = jnp.dot(layout, normed, preferred_element_type=f32).astype(bf16)
    leaving = leaving.reshape(sends, 2, model_width)
    arrived = lax.all_to_all(leaving, ("y", "x", "c"), split_axis=0, concat_axis=0, tiled=True)
    summed = experts(arrived.reshape(2 * sends, model_width), gate_up, down)
    summed = summed.reshape(sends, 2, model_width)
    returned = lax.all_to_all(summed, ("y", "x", "c"), split_axis=0, concat_axis=0, tiled=True)
    results = returned.reshape(2 * sends, model_width)
    picked = jnp.take(results, target.reshape(-1), axis=0)
    picked = picked.reshape(rows_here, chosen, model_width).astype(f32)
    combined = jnp.sum(route_weights[:, :, None] * picked, axis=1)
    return (widened + combined).astype(bf16)


def solution(mesh):
    split = Mesh(mesh.devices.reshape(N4, N4, NZ, 2), ALL)
    placed = (
        P(SP, TP, None),
        P(SP, TP, None),
        P(SP, TP, None),
        P(SP, TP, None),
        P(SP, TP, None),
        P(SP, TP, None),
        P(None, TP),
        P(),
        P(),
        P(TP, None),
        P(TP, None),
        P(ALL, None),
        P(),
        P(ALL, None),
        P(ALL, None),
        P(SP, None, TP),
        P(SP, None, TP),
        P(SP, TP, None),
    )

    return jax.shard_map(
        per_device, mesh=split, in_specs=placed, out_specs=P(ALL, None), check_vma=False
    )
```

```python
import functools

import jax
import jax.numpy as jnp
from jax import lax
from jax.experimental import pallas as pl
from jax.experimental.pallas import tpu as pltpu
from jax.sharding import Mesh
from jax.sharding import PartitionSpec as P


TP = ("z", "c")
SP = ("y", "x")
ALL = ("y", "x", "z", "c")

EPSILON = 1e-06
LIMIT = 7.0
SLOPE = 1.702
LOG2E = 1.4426950408889634

N4 = 4
NZ = 8
TOK = 256
KEYS = N4 * TOK
CHUNK = 128
STAT = 16
DA = 128
DB = 64
VA = 256
VB = 128
f32 = jnp.float32
bf16 = jnp.bfloat16


def shifted(array, axis, count, by):
    return lax.ppermute(array, axis, [(i, (i + by) % count) for i in range(count)])


def one_group(q_scr, k_scr, v_scr, o_scr, block, row, width, packed):
    rows = pl.ds(pl.multiple_of(row * CHUNK, CHUNK), CHUNK)
    q = q_scr[block, rows, :]
    value_width = v_scr.shape[1]
    scaling = width ** (-0.5) * LOG2E
    lane = lax.broadcasted_iota(jnp.int32, (CHUNK, 128), 1)
    stats = jnp.zeros((CHUNK, 128), f32)
    for which in range(2):
        if packed:
            mine = lax.broadcasted_iota(jnp.int32, q.shape, 1) // width == which
            part = jnp.where(mine, q, jnp.zeros_like(q))
            keys = k_scr[...]
        else:
            part = q[:, which * width : (which + 1) * width]
            keys = k_scr[:, which * width : (which + 1) * width]
        scores = (
            lax.dot_general(part, keys, (((1,), (1,)), ((), ())), preferred_element_type=f32)
            * scaling
        )
        highest = jnp.max(scores, axis=1, keepdims=True).astype(bf16).astype(f32)
        expo = jnp.exp2(scores - highest)
        total = jnp.sum(expo, axis=1, keepdims=True)
        carried = jnp.dot(expo.astype(bf16), v_scr[...], preferred_element_type=f32)
        o_scr[block, rows, which * value_width : (which + 1) * value_width] = carried.astype(bf16)
        coarse = total.astype(bf16).astype(f32)
        for at, stat in enumerate((highest, coarse, total - coarse)):
            stats = jnp.where(lane == 3 * which + at, stat, stats)
    o_scr[block, TOK : TOK + STAT, rows] = stats.T[:STAT, :].astype(bf16)


def partial_kernel(blocks, *refs):
    xs, ys = refs[:4], refs[4:8]
    count = len(blocks)
    outs_a, outs_b = refs[8 : 8 + count], refs[8 + count : 8 + 2 * count]
    qa, ka, va, oa, qb, kb, vb, ob = refs[8 + 2 * count :]
    for i in range(4):
        rows = slice(i * TOK, (i + 1) * TOK)
        ka[rows, :] = xs[i][:, : 2 * DA]
        va[rows, :] = xs[i][:, 2 * DA : 2 * DA + VA]
        kb[rows, :] = ys[i][:, : 2 * DB]
        vb[rows, :] = ys[i][:, 2 * DB : 2 * DB + VB]
    for at, i in enumerate(blocks):
        qa[at] = ys[i][:, 2 * DB + VB :]
        qb[at] = xs[i][:, 2 * DA + VA :]
        oa[at, TOK:, :] = jnp.zeros((STAT, 2 * VA), bf16)
        ob[at, TOK:, :] = jnp.zeros((STAT, 2 * VB), bf16)
    per = TOK // CHUNK

    def step(n, carry):
        block, row = n // per, n % per
        one_group(qa, ka, va, oa, block, row, DA, False)
        one_group(qb, kb, vb, ob, block, row, DB, True)
        return carry

    lax.fori_loop(0, count * per, step, 0)
    for at in range(count):
        outs_a[at][...] = oa[at]
        outs_b[at][...] = ob[at]


def partial_attention(xs, ys, blocks):
    count = len(blocks)
    vmem = pl.BlockSpec(memory_space=pltpu.VMEM)
    shapes = [jax.ShapeDtypeStruct((TOK + STAT, 2 * VA), bf16)] * count
    shapes += [jax.ShapeDtypeStruct((TOK + STAT, 2 * VB), bf16)] * count
    outs = pl.pallas_call(
        functools.partial(partial_kernel, blocks),
        out_shape=shapes,
        in_specs=[vmem] * 8,
        out_specs=[vmem] * (2 * count),
        scratch_shapes=[
            pltpu.VMEM((count, TOK, 2 * DA), bf16),
            pltpu.VMEM((KEYS, 2 * DA), bf16),
            pltpu.VMEM((KEYS, VA), bf16),
            pltpu.VMEM((count, TOK + STAT, 2 * VA), bf16),
            pltpu.VMEM((count, TOK, 2 * DB), bf16),
            pltpu.VMEM((KEYS, 2 * DB), bf16),
            pltpu.VMEM((KEYS, VB), bf16),
            pltpu.VMEM((count, TOK + STAT, 2 * VB), bf16),
        ],
        cost_estimate=pl.CostEstimate(
            flops=count * 604_000_000, bytes_accessed=4_000_000, transcendentals=count * 1_048_576
        ),
    )(*xs, *ys)
    return outs[:count], outs[count:]


def merge_group(parts, stat_scr, rows, value_width, weight, gain):
    lanes = stat_scr[rows, :]
    column = lambda part, at: lanes[:, STAT * part + at : STAT * part + at + 1]
    heard = []
    for which in range(2):
        maxima = [column(i, 3 * which) for i in range(4)]
        highest = jnp.maximum(jnp.maximum(maxima[0], maxima[1]), jnp.maximum(maxima[2], maxima[3]))
        total, summed = 0.0, 0.0
        for i in range(4):
            factor = jnp.exp2(maxima[i] - highest)
            total = total + factor * (column(i, 3 * which + 1) + column(i, 3 * which + 2))
            values = parts[i][rows, which * value_width : (which + 1) * value_width]
            summed = summed + factor * values.astype(f32)
        heard.append(summed / total)
    differ = heard[0] - weight * heard[1]
    scaled = lax.rsqrt(jnp.mean(differ * differ, axis=1, keepdims=True) + EPSILON)
    return (differ * scaled * gain).astype(bf16)


def merge_kernel(core, lam, gain_a, gain_b, *refs):
    pa, pb = refs[:4], refs[4:8]
    away, mine, sa, sb, att = refs[-5:]
    for parts, scr in ((pa, sa), (pb, sb)):
        rows = [p[TOK:, :TOK].astype(f32) for p in parts]
        rows.append(jnp.zeros((128 - 4 * STAT, TOK), f32))
        scr[...] = jnp.concatenate(rows, axis=0).T

    def step(n, carry):
        rows = pl.ds(pl.multiple_of(n * 64, 64), 64)
        att[rows, :VA] = merge_group(pa, sa, rows, VA, lam[0], gain_a[...])
        att[rows, VA:] = merge_group(pb, sb, rows, VB, lam[1], gain_b[...])
        return carry

    lax.fori_loop(0, TOK // 64, step, 0)
    half = TOK // 2
    me = core[0]
    away[...] = att[pl.ds(pl.multiple_of((1 - me) * half, half), half), :]
    mine[...] = att[pl.ds(pl.multiple_of(me * half, half), half), :]


def merged(parts_a, parts_b, lam, gain_a, gain_b, core, first):
    smem = pl.BlockSpec(memory_space=pltpu.SMEM)
    vmem = pl.BlockSpec(memory_space=pltpu.VMEM)
    out = jax.ShapeDtypeStruct((TOK // 2, VA + VB), bf16)
    return pl.pallas_call(
        merge_kernel,
        out_shape=[out, out],
        in_specs=[smem, smem] + [vmem] * 10 + [pl.BlockSpec(memory_space=pl.ANY)] * len(first),
        out_specs=[vmem, vmem],
        scratch_shapes=[
            pltpu.VMEM((TOK, 128), f32),
            pltpu.VMEM((TOK, 128), f32),
            pltpu.VMEM((TOK, VA + VB), bf16),
        ],
        cost_estimate=pl.CostEstimate(
            flops=800_000_000, bytes_accessed=2_000_000, transcendentals=20_000
        ),
        name="merge_parts",
    )(
        core.reshape(1),
        lam,
        gain_a.reshape(1, -1),
        gain_b.reshape(1, -1),
        *parts_a,
        *parts_b,
        *first,
    )


def project_kernel(mine, joined, wa, wb, xa, xb, out):
    total = jnp.dot(mine[:, :VA], wa[...], preferred_element_type=f32)
    total += jnp.dot(joined[:, :VA], xa[...], preferred_element_type=f32)
    total += jnp.dot(mine[:, VA:], wb[...], preferred_element_type=f32)
    total += jnp.dot(joined[:, VA:], xb[...], preferred_element_type=f32)
    out[...] = total.astype(bf16)


def project(mine, joined, wa, wb, xa, xb):
    width, tile = wa.shape[1], 1024
    whole = pl.BlockSpec(mine.shape, lambda i: (0, 0))
    deep = pl.BlockSpec((VA, tile), lambda i: (0, i))
    flat = pl.BlockSpec((VB, tile), lambda i: (0, i))
    return pl.pallas_call(
        project_kernel,
        grid=(width // tile,),
        out_shape=jax.ShapeDtypeStruct((mine.shape[0], width), bf16),
        in_specs=[whole, whole, deep, flat, deep, flat],
        out_specs=pl.BlockSpec((mine.shape[0], tile), lambda i: (0, i)),
        cost_estimate=pl.CostEstimate(
            flops=3_000_000_000, bytes_accessed=8_000_000, transcendentals=0
        ),
        name="project",
    )(mine, joined, wa, wb, xa, xb)


def sum_over_z(own):
    pieces = lax.all_to_all(own, "z", split_axis=0, concat_axis=0, tiled=True)
    return jnp.sum(pieces.astype(f32), axis=0)


def attention(query_a, key_a, value_a, query_b, key_b, value_b, lambdas, gain_a, gain_b, out_a, out_b, first):
    flat = lambda a: a.reshape(TOK, -1)
    by_core = lambda a: jnp.swapaxes(a.reshape(NZ, 2, 16, -1), 0, 1).reshape(TOK, -1)
    for_x = jnp.concatenate([flat(key_a), flat(value_a), by_core(query_b)], axis=1)
    for_y = jnp.concatenate([flat(key_b), flat(value_b), by_core(query_a)], axis=1)
    order = (2, 1, 3)
    got_x = {k: shifted(for_x, "x", N4, k) for k in order}
    got_y = {k: shifted(for_y, "y", N4, k) for k in order}
    xs = [for_x] + [got_x[k] for k in (1, 2, 3)]
    ys = [for_y] + [got_y[k] for k in (1, 2, 3)]
    far_a, far_b = partial_attention(xs, ys, order)
    back = {}
    for at, k in enumerate(order):
        back[k] = (shifted(far_a[at], "y", N4, -k), shifted(far_b[at], "x", N4, -k))
    own_a, own_b = partial_attention(xs, ys, (0,))
    parts_a = [own_a[0]] + [back[k][0] for k in (1, 2, 3)]
    parts_b = [own_b[0]] + [back[k][1] for k in (1, 2, 3)]
    core = lax.axis_index("c").astype(jnp.int32)
    away, mine = merged(parts_a, parts_b, lambdas.reshape(-1), gain_a, gain_b, core, first)
    other_a, other_b = shifted(out_a, "c", 2, 1), shifted(out_b, "c", 2, 1)
    own = project(mine, shifted(away, "c", 2, 1), out_a, out_b, other_a, other_b)
    return sum_over_z(own.reshape(NZ, 16, -1))


OFFSETS = (0, -1, 1, -2, 2, -3, 3, 4)
STEP = 512
RING = 2560
CROSS = ("y", "x", "c")


def gate_kernel(*refs):
    *pieces, weights, out, tokens = refs
    rows = pieces[0].shape[0]
    for at, piece in enumerate(pieces):
        tokens[at * rows : (at + 1) * rows, :] = piece[...]
    out[...] = jnp.zeros_like(out)

    def step(n, carry):
        part = pl.ds(pl.multiple_of(n * STEP, STEP), STEP)
        out[...] += jnp.dot(tokens[:, part], weights[part, :], preferred_element_type=f32)
        return carry

    lax.fori_loop(0, weights.shape[0] // STEP, step, 0)


def gate_sums(pieces, weights):
    vmem = pl.BlockSpec(memory_space=pltpu.VMEM)
    rows = len(pieces) * pieces[0].shape[0]
    depth, both = weights.shape
    return pl.pallas_call(
        gate_kernel,
        out_shape=jax.ShapeDtypeStruct((rows, both), f32),
        in_specs=[vmem] * (len(pieces) + 1),
        out_specs=vmem,
        scratch_shapes=[pltpu.VMEM((rows, depth), bf16)],
        cost_estimate=pl.CostEstimate(
            flops=max(8 * rows * depth * both, 3_000_000_000),
            bytes_accessed=4_000_000,
            transcendentals=0,
        ),
    )(*pieces, weights)


def experts(block, crossing, weights):
    gate_a, gate_b, down_a, down_b = weights
    rows, _ = block.shape
    ring = {0: block}
    for k in range(1, 5):
        ring[k] = shifted(ring[k - 1], "z", NZ, 1)
        if k < 4:
            ring[-k] = shifted(ring[1 - k], "z", NZ, -1)
    sums = []
    for offsets in (OFFSETS[:5], OFFSETS[5:7], (-4,)):
        sums.append(gate_sums([ring[-k] for k in offsets], gate_a))
    swapped = lambda a, n, m: jnp.swapaxes(a.reshape(n, m, 2, -1), 0, 1).reshape(a.shape)
    cross = jnp.dot(crossing, gate_b, preferred_element_type=f32)
    both = jnp.concatenate(sums, axis=0) + swapped(cross, rows // 2, NZ)
    units = both.shape[1] // 2
    gate = jnp.minimum(both[:, :units], LIMIT)
    upward = jnp.clip(both[:, units:], -LIMIT, LIMIT) + 1.0
    active = (gate * jax.nn.sigmoid(SLOPE * gate) * upward).astype(bf16)

    def share(offset):
        at = OFFSETS.index(4 if offset == -4 else offset) * rows
        return jnp.dot(active[at : at + rows], down_a, preferred_element_type=f32)

    carried = {}
    for k in range(4, 0, -1):
        for sign in (-1, 1):
            if k == 4 and sign == 1:
                continue
            part = share(sign * k)
            if sign in carried:
                part = part + carried[sign].astype(f32)
            carried[sign] = shifted(part.astype(bf16), "z", NZ, sign)
    total = (share(0) + carried[-1].astype(f32) + carried[1].astype(f32)).astype(bf16)
    leaving = jnp.dot(swapped(active, NZ, rows // 2), down_b, preferred_element_type=f32)
    return total, leaving.astype(bf16)


def pack_kernel(core, *refs):
    ins, (both, lower) = refs[:6], refs[6:]
    units = ins[0].shape[2]
    for at in range(4):
        both[:, at * units : (at + 1) * units] = ins[at][0]
    for at in range(2):
        lower[at * units : (at + 1) * units, :] = ins[4 + at][0]


def packed(arrays, core, start, width):
    units, tile = arrays[0].shape[2], STEP
    steps, first = width // tile, start // tile
    deep = pl.BlockSpec((1, tile, units), lambda i, c: (c[0], i + first, 0))
    flat = pl.BlockSpec((1, units, tile), lambda i, c: (c[0], 0, i + first))
    return pl.pallas_call(
        pack_kernel,
        grid_spec=pltpu.PrefetchScalarGridSpec(
            num_scalar_prefetch=1,
            grid=(steps,),
            in_specs=[deep] * 4 + [flat] * 2,
            out_specs=[
                pl.BlockSpec((tile, 4 * units), lambda i, c: (i, 0)),
                pl.BlockSpec((2 * units, tile), lambda i, c: (0, i)),
            ],
        ),
        out_shape=[
            jax.ShapeDtypeStruct((width, 4 * units), bf16),
            jax.ShapeDtypeStruct((2 * units, width), bf16),
        ],
        cost_estimate=pl.CostEstimate(
            flops=2_000_000_000, bytes_accessed=3000 * width, transcendentals=0
        ),
    )(core.reshape(1), *arrays)


def expert_weights(w_gate, w_up, w_down, core):
    other = lambda w: shifted(w, "c", 2, 1)
    arrays = [w_gate, other(w_gate), w_up, other(w_up), w_down, other(w_down)]
    gate_a, down_a = packed(arrays, core, 0, RING)
    gate_b, down_b = packed(arrays, core, RING, w_gate.shape[1] - RING)
    return gate_a, gate_b, down_a, down_b


def slots_of(ids):
    flat = ids.reshape(-1)
    same = (flat[:, None] == flat[None, :]).astype(jnp.int32)
    place = jnp.sum(same * jnp.tril(jnp.ones_like(same), -1), axis=1)
    return (flat * 2 + place).reshape(ids.shape)


def per_device(
    query_a,
    key_a,
    value_a,
    query_b,
    key_b,
    value_b,
    lambdas,
    gain_a,
    gain_b,
    out_a,
    out_b,
    residual,
    norm_gain,
    route_ids,
    route_weights,
    w_gate,
    w_up,
    w_down,
):
    core = lax.axis_index("c").astype(jnp.int32)
    z = lax.axis_index("z").astype(jnp.int32)
    weights = expert_weights(w_gate, w_up, w_down, core)
    target = slots_of(route_ids)
    rows_here, chosen = route_ids.shape
    model_width = residual.shape[1]
    sends = 2 * N4 * N4
    width = model_width - RING
    across = lambda a: lax.all_to_all(a, CROSS, split_axis=0, concat_axis=0, tiled=True)
    along = lambda a: lax.all_to_all(a, "z", split_axis=0, concat_axis=0, tiled=True)
    slots = jnp.arange(2 * sends, dtype=jnp.int32)
    layout = jnp.any(target[None, :, :] == slots[:, None, None], axis=2).astype(bf16)
    taken = target[:, :, None] == slots[None, None, :]
    shares = jnp.sum(jnp.where(taken, route_weights[:, :, None], 0.0), axis=1)
    coarse = shares.astype(bf16).astype(f32)
    beside = [jnp.any(taken, axis=1).astype(f32), coarse, shares - coarse, jnp.zeros_like(shares)]
    beside = jnp.concatenate(beside, axis=1).astype(bf16)
    projected = attention(
        query_a,
        key_a,
        value_a,
        query_b,
        key_b,
        value_b,
        lambdas,
        gain_a,
        gain_b,
        out_a,
        out_b,
        (layout, beside),
    )
    mixed = (residual.astype(f32) + projected).astype(bf16)
    widened = mixed.astype(f32)
    normed = (
        widened
        * lax.rsqrt(jnp.mean(widened * widened, axis=1, keepdims=True) + EPSILON)
        * norm_gain
    ).astype(bf16)
    leaving = jnp.dot(layout, normed[:, :RING], preferred_element_type=f32).astype(bf16)
    arrived = across(leaving.reshape(sends, 2, RING))
    sent = jnp.concatenate([normed[:, RING:], beside], axis=1)
    tokens = along(jnp.broadcast_to(sent[None], (NZ, *sent.shape)))
    count = NZ * rows_here
    tokens = tokens.reshape(count, sent.shape[1])
    wide = jnp.arange(2 * sends * NZ, dtype=jnp.int32)[None, :]
    offset = wide // 2 % NZ
    home = sum(jnp.where(offset == at, k, 0) for at, k in enumerate(OFFSETS))
    token = jnp.arange(count, dtype=jnp.int32)[:, None]
    near = (home + z + NZ) % NZ == token // rows_here
    spread = (wide // (2 * NZ) * 2 + wide % 2 == slots[:, None]).astype(bf16)
    extra = tokens[:, width:].reshape(count, 4, 2 * sends)
    extra = [
        jnp.where(near, jnp.dot(extra[:, k], spread, preferred_element_type=f32), 0.0).astype(bf16)
        for k in range(3)
    ]
    crossing = lax.dot_general(
        extra[0], tokens[:, :width], (((0,), (0,)), ((), ())), preferred_element_type=f32
    ).astype(bf16)
    crossing = across(crossing.reshape(sends, 2 * NZ, width))
    total, leaving = experts(
        arrived.reshape(2 * sends, RING), crossing.reshape(sends * NZ * 2, width), weights
    )
    leaving = across(leaving.reshape(sends, 2 * NZ, width)).reshape(sends * NZ * 2, width)
    parts = jnp.dot(
        jnp.concatenate(extra[1:], axis=0), leaving, preferred_element_type=f32
    )
    parts = (parts[:count] + parts[count:]).astype(bf16)
    parts = along(parts.reshape(NZ, rows_here, width))
    upper = jnp.sum(parts.astype(f32), axis=0)
    results = across(total.reshape(sends, 2, RING)).reshape(2 * sends, RING)
    picked = jnp.take(results, target.reshape(-1), axis=0)
    picked = picked.reshape(rows_here, chosen, RING).astype(f32)
    lower = jnp.sum(route_weights[:, :, None] * picked, axis=1)
    return (widened + jnp.concatenate([lower, upper], axis=1)).astype(bf16)


def solution(mesh):
    split = Mesh(mesh.devices.reshape(N4, N4, NZ, 2), ALL)
    placed = (
        P(SP, TP, None),
        P(SP, TP, None),
        P(SP, TP, None),
        P(SP, TP, None),
        P(SP, TP, None),
        P(SP, TP, None),
        P(None, TP),
        P(),
        P(),
        P(TP, None),
        P(TP, None),
        P(ALL, None),
        P(),
        P(ALL, None),
        P(ALL, None),
        P(SP, None, TP),
        P(SP, None, TP),
        P(SP, TP, None),
    )

    return jax.shard_map(
        per_device, mesh=split, in_specs=placed, out_specs=P(ALL, None), check_vma=False
    )
```

```python
import functools

import jax
import jax.numpy as jnp
from jax import lax
from jax.experimental import pallas as pl
from jax.experimental.pallas import tpu as pltpu
from jax.sharding import Mesh
from jax.sharding import PartitionSpec as P


TP = ("z", "c")
SP = ("y", "x")
ALL = ("y", "x", "z", "c")

EPSILON = 1e-06
LIMIT = 7.0
SLOPE = 1.702
LOG2E = 1.4426950408889634

N4 = 4
NZ = 8
TOK = 256
CHUNK = 128
STAT = 16
DA = 128
DB = 64
VA = 256
VB = 128
f32 = jnp.float32
bf16 = jnp.bfloat16


def shifted(array, axis, count, by):
    return lax.ppermute(array, axis, [(i, (i + by) % count) for i in range(count)])


def one_group(q_ref, q_at, sources, k_at, out, half, width, value_width):
    rows = [
        q_ref[pl.ds(pl.multiple_of(z * 32 + half * 16, 16), 16), q_at : q_at + 2 * width]
        for z in range(NZ)
    ]
    q = jnp.concatenate(rows, axis=0)
    here = pl.ds(pl.multiple_of(half * CHUNK, CHUNK), CHUNK)
    scaling = width ** (-0.5) * LOG2E
    lane = lax.broadcasted_iota(jnp.int32, (CHUNK, 128), 1)
    stats = jnp.zeros((CHUNK, 128), f32)
    v_at = k_at + 2 * width
    for which in range(2):
        if width < 128:
            mine = lax.broadcasted_iota(jnp.int32, q.shape, 1) // width == which
            part = jnp.where(mine, q, jnp.zeros_like(q))
            keys = slice(k_at, k_at + 2 * width)
        else:
            part = q[:, which * width : (which + 1) * width]
            keys = slice(k_at + which * width, k_at + (which + 1) * width)
        scores = [
            lax.dot_general(
                part, ref[:, keys], (((1,), (1,)), ((), ())), preferred_element_type=f32
            )
            for ref in sources
        ]
        scores = jnp.concatenate(scores, axis=1) * scaling
        highest = jnp.max(scores, axis=1, keepdims=True).astype(bf16).astype(f32)
        expo = jnp.exp2(scores - highest)
        total = jnp.sum(expo, axis=1, keepdims=True)
        expo = expo.astype(bf16)
        carried = sum(
            jnp.dot(
                expo[:, i * TOK : (i + 1) * TOK],
                ref[:, v_at : v_at + value_width],
                preferred_element_type=f32,
            )
            for i, ref in enumerate(sources)
        )
        out[here, which * value_width : (which + 1) * value_width] = carried.astype(bf16)
        coarse = total.astype(bf16).astype(f32)
        for at, stat in enumerate((highest, coarse, total - coarse)):
            stats = jnp.where(lane == 3 * which + at, stat, stats)
    out[TOK : TOK + STAT, here] = stats.T[:STAT, :].astype(bf16)


def partial_kernel(*refs):
    xs, ys, (q_a, q_b, out_a, out_b) = refs[:4], refs[4:8], refs[8:]
    out_a[TOK:, :] = jnp.zeros((STAT, 2 * VA), bf16)

    def step(half, carry):
        one_group(q_a, 2 * DB + VB, xs, 0, out_a, half, DA, VA)
        one_group(q_b, 2 * DA + VA, ys, 0, out_b, half, DB, VB)
        return carry

    lax.fori_loop(0, 2, step, 0)


def partial_attention(xs, ys, block):
    vmem = pl.BlockSpec(memory_space=pltpu.VMEM)
    return pl.pallas_call(
        partial_kernel,
        out_shape=[
            jax.ShapeDtypeStruct((TOK + STAT, 2 * VA), bf16),
            jax.ShapeDtypeStruct((TOK + STAT, 2 * VB), bf16),
        ],
        in_specs=[vmem] * 10,
        out_specs=[vmem] * 2,
        cost_estimate=pl.CostEstimate(
            flops=1_500_000_000, bytes_accessed=3_000_000, transcendentals=1_048_576
        ),
        name="partial_attention",
    )(*xs, *ys, ys[block], xs[block])


def merge_group(parts, stat_scr, rows, value_width, weight, gain):
    lanes = stat_scr[rows, :]
    column = lambda part, at: lanes[:, STAT * part + at : STAT * part + at + 1]
    heard = []
    for which in range(2):
        maxima = [column(i, 3 * which) for i in range(4)]
        highest = jnp.maximum(jnp.maximum(maxima[0], maxima[1]), jnp.maximum(maxima[2], maxima[3]))
        total, summed = 0.0, 0.0
        for i in range(4):
            factor = jnp.exp2(maxima[i] - highest)
            total = total + factor * (column(i, 3 * which + 1) + column(i, 3 * which + 2))
            values = parts[i][rows, which * value_width : (which + 1) * value_width]
            summed = summed + factor * values.astype(f32)
        heard.append(summed / total)
    differ = heard[0] - weight * heard[1]
    scaled = lax.rsqrt(jnp.mean(differ * differ, axis=1, keepdims=True) + EPSILON)
    return (differ * scaled * gain).astype(bf16)


def merge_kernel(core, lam, gain_a, gain_b, *refs):
    pa, pb = refs[:4], refs[4:8]
    away, mine, sa, sb, att = refs[-5:]
    for parts, scr in ((pa, sa), (pb, sb)):
        rows = [p[TOK:, :TOK].astype(f32) for p in parts]
        rows.append(jnp.zeros((128 - 4 * STAT, TOK), f32))
        scr[...] = jnp.concatenate(rows, axis=0).T

    def step(n, carry):
        rows = pl.ds(pl.multiple_of(n * 64, 64), 64)
        att[rows, :VA] = merge_group(pa, sa, rows, VA, lam[0], gain_a[...])
        att[rows, VA:] = merge_group(pb, sb, rows, VB, lam[1], gain_b[...])
        return carry

    lax.fori_loop(0, TOK // 64, step, 0)
    half = TOK // 2
    me = core[0]
    away[...] = att[pl.ds(pl.multiple_of((1 - me) * half, half), half), :]
    mine[...] = att[pl.ds(pl.multiple_of(me * half, half), half), :]


def merged(parts_a, parts_b, lam, gain_a, gain_b, core, first):
    smem = pl.BlockSpec(memory_space=pltpu.SMEM)
    vmem = pl.BlockSpec(memory_space=pltpu.VMEM)
    out = jax.ShapeDtypeStruct((TOK // 2, VA + VB), bf16)
    return pl.pallas_call(
        merge_kernel,
        out_shape=[out, out],
        in_specs=[smem, smem] + [vmem] * 10 + [pl.BlockSpec(memory_space=pl.ANY)] * len(first),
        out_specs=[vmem, vmem],
        scratch_shapes=[
            pltpu.VMEM((TOK, 128), f32),
            pltpu.VMEM((TOK, 128), f32),
            pltpu.VMEM((TOK, VA + VB), bf16),
        ],
        cost_estimate=pl.CostEstimate(
            flops=800_000_000, bytes_accessed=2_000_000, transcendentals=20_000
        ),
        name="merge_parts",
    )(
        core.reshape(1),
        lam,
        gain_a.reshape(1, -1),
        gain_b.reshape(1, -1),
        *parts_a,
        *parts_b,
        *first,
    )


def project_kernel(mine, joined, wa, wb, xa, xb, out):
    total = jnp.dot(mine[:, :VA], wa[...], preferred_element_type=f32)
    total += jnp.dot(joined[:, :VA], xa[...], preferred_element_type=f32)
    total += jnp.dot(mine[:, VA:], wb[...], preferred_element_type=f32)
    total += jnp.dot(joined[:, VA:], xb[...], preferred_element_type=f32)
    out[...] = total.astype(bf16)


def project(mine, joined, wa, wb, xa, xb):
    width, tile = wa.shape[1], 1024
    whole = pl.BlockSpec(mine.shape, lambda i: (0, 0))
    deep = pl.BlockSpec((VA, tile), lambda i: (0, i))
    flat = pl.BlockSpec((VB, tile), lambda i: (0, i))
    return pl.pallas_call(
        project_kernel,
        grid=(width // tile,),
        out_shape=jax.ShapeDtypeStruct((mine.shape[0], width), bf16),
        in_specs=[whole, whole, deep, flat, deep, flat],
        out_specs=pl.BlockSpec((mine.shape[0], tile), lambda i: (0, i)),
        cost_estimate=pl.CostEstimate(
            flops=3_000_000_000, bytes_accessed=8_000_000, transcendentals=0
        ),
        name="project",
    )(mine, joined, wa, wb, xa, xb)


def sum_over_z(own):
    pieces = lax.all_to_all(own, "z", split_axis=0, concat_axis=0, tiled=True)
    return jnp.sum(pieces.astype(f32), axis=0)


def attention(query_a, key_a, value_a, query_b, key_b, value_b, lambdas, gain_a, gain_b, out_a, out_b, first):
    flat = lambda a: a.reshape(TOK, -1)
    for_x = jnp.concatenate([flat(key_a), flat(value_a), flat(query_b)], axis=1)
    for_y = jnp.concatenate([flat(key_b), flat(value_b), flat(query_a)], axis=1)
    order = (2, 1, 3)
    got_x = {k: shifted(for_x, "x", N4, k) for k in order}
    got_y = {k: shifted(for_y, "y", N4, k) for k in order}
    xs = [for_x] + [got_x[k] for k in (1, 2, 3)]
    ys = [for_y] + [got_y[k] for k in (1, 2, 3)]
    parts, back = {}, {}
    for k in (*order, 0):
        parts[k] = partial_attention(xs, ys, k)
        if k:
            back[k] = shifted(parts[k][0], "y", N4, -k), shifted(parts[k][1], "x", N4, -k)
    parts_a = [parts[0][0]] + [back[k][0] for k in (1, 2, 3)]
    parts_b = [parts[0][1]] + [back[k][1] for k in (1, 2, 3)]
    core = lax.axis_index("c").astype(jnp.int32)
    away, mine = merged(parts_a, parts_b, lambdas.reshape(-1), gain_a, gain_b, core, first)
    other_a, other_b = shifted(out_a, "c", 2, 1), shifted(out_b, "c", 2, 1)
    own = project(mine, shifted(away, "c", 2, 1), out_a, out_b, other_a, other_b)
    return sum_over_z(own.reshape(NZ, 16, -1))


HALVES = 2
STEP = 1024


def gate_kernel(count, *refs):
    outs, (tokens, sums) = refs[-2 - count : -2], refs[-2:]
    pieces, weights = refs[: -3 - count], refs[-3 - count]
    rows = outs[0].shape[0]
    halves = []
    for piece in pieces:
        halves += [piece] if len(piece.shape) == 2 else [piece.at[h] for h in range(HALVES)]
    for at, half in enumerate(halves):
        row, column = at // HALVES * rows, at % HALVES * half.shape[1]
        tokens[row : row + rows, column : column + half.shape[1]] = half[...]
    sums[...] = jnp.zeros_like(sums)

    def step(n, carry):
        part = pl.ds(pl.multiple_of(n * STEP, STEP), STEP)
        sums[...] += jnp.dot(tokens[:, part], weights[part, :], preferred_element_type=f32)
        return carry

    lax.fori_loop(0, weights.shape[0] // STEP, step, 0)
    units = outs[0].shape[1]
    for at, out in enumerate(outs):
        here = slice(at * rows, (at + 1) * rows)
        gate = jnp.minimum(sums[here, :units], LIMIT)
        upward = jnp.clip(sums[here, units:], -LIMIT, LIMIT) + 1.0
        out[...] = (gate * jax.nn.sigmoid(SLOPE * gate) * upward).astype(bf16)


def gated_units(blocks, weights):
    vmem = pl.BlockSpec(memory_space=pltpu.VMEM)
    pieces = [piece for block in blocks for piece in block]
    count, rows = len(blocks), pieces[0].shape[-2]
    depth, both = weights.shape
    return pl.pallas_call(
        functools.partial(gate_kernel, count),
        out_shape=[jax.ShapeDtypeStruct((rows, both // 2), bf16)] * count,
        in_specs=[vmem] * (len(pieces) + 1),
        out_specs=[vmem] * count,
        scratch_shapes=[
            pltpu.VMEM((count * rows, depth), bf16),
            pltpu.VMEM((count * rows, both), f32),
        ],
        cost_estimate=pl.CostEstimate(
            flops=4_000_000_000, bytes_accessed=6_000_000, transcendentals=count * rows * 256
        ),
    )(*pieces, weights)


def experts(block, gate_up, downs):
    ring = {0: block}
    for k in range(1, 5):
        for sign in (1, -1):
            if k < 3:
                ring[sign * k] = shifted(ring[sign * (k - 1)], "z", NZ, sign)
                continue
            for h in range(HALVES):
                if k == 4 and h == (sign < 0) or k == 3:
                    held = ring[2 * sign][h] if k == 3 else ring[3 * sign, h]
                    ring[sign * k, h] = shifted(held, "z", NZ, sign)
    ring[4, 1] = ring[-4, 1]
    pieces = lambda k: [ring[k]] if k in ring else [ring[k, h] for h in range(HALVES)]
    units = {}
    for offsets in ((0,), (1, -1), (2, -2), (3, -3), (4,)):
        outs = gated_units([pieces(k) for k in offsets], gate_up)
        for k, out in zip(offsets, outs):
            units[-k] = out
    units[4] = units[-4]

    def share(offset, h):
        return jnp.dot(units[offset], downs[h], preferred_element_type=f32)

    carried = {}
    for k in range(4, 0, -1):
        for h in range(HALVES):
            for sign, start in ((-1, 4 - h), (1, 3 + h)):
                if k > start:
                    continue
                part = share(sign * k, h)
                if k < start:
                    part = part + carried[sign, h].astype(f32)
                carried[sign, h] = shifted(part.astype(bf16), "z", NZ, sign)
    total = []
    for h in range(HALVES):
        part = share(0, h) + carried[-1, h].astype(f32) + carried[1, h].astype(f32)
        total.append(part.astype(bf16))
    return jnp.concatenate(total, axis=1)


def pack_kernel(core, gate, gate_other, upward, upward_other, *refs):
    downs, (both, *lowers) = refs[:4], refs[4:]
    units = gate.shape[2]
    for at, ref in enumerate((gate, gate_other, upward, upward_other)):
        both[:, at * units : (at + 1) * units] = ref[0]
    for h, lower in enumerate(lowers):
        for at in range(2):
            lower[at * units : (at + 1) * units, :] = downs[2 * h + at][0]


def expert_weights(w_gate, w_up, w_down, core):
    _, depth, units = w_gate.shape
    tile = 512
    deep = pl.BlockSpec((1, tile, units), lambda i, c: (c[0], i, 0))
    steps = depth // tile
    thin = tile // HALVES
    flat = [
        pl.BlockSpec((1, units, thin), lambda i, c, h=h: (c[0], 0, i + h * steps))
        for h in range(HALVES)
    ]
    other = lambda w: shifted(w, "c", 2, 1)
    return pl.pallas_call(
        pack_kernel,
        grid_spec=pltpu.PrefetchScalarGridSpec(
            num_scalar_prefetch=1,
            grid=(depth // tile,),
            in_specs=[deep] * 4 + [flat[0]] * 2 + [flat[1]] * 2,
            out_specs=[
                pl.BlockSpec((tile, 4 * units), lambda i, c: (i, 0)),
                *[pl.BlockSpec((2 * units, thin), lambda i, c: (0, i))] * HALVES,
            ],
        ),
        out_shape=[
            jax.ShapeDtypeStruct((depth, 4 * units), bf16),
            *[jax.ShapeDtypeStruct((2 * units, depth // HALVES), bf16)] * HALVES,
        ],
        cost_estimate=pl.CostEstimate(
            flops=3_000_000_000, bytes_accessed=12_000_000, transcendentals=0
        ),
        name="pack_weights",
    )(core.reshape(1), w_gate, other(w_gate), w_up, other(w_up), *[w_down, other(w_down)] * HALVES)


def slots_of(ids):
    flat = ids.reshape(-1)
    same = (flat[:, None] == flat[None, :]).astype(jnp.int32)
    place = jnp.sum(same * jnp.tril(jnp.ones_like(same), -1), axis=1)
    return (flat * 2 + place).reshape(ids.shape)


def per_device(
    query_a,
    key_a,
    value_a,
    query_b,
    key_b,
    value_b,
    lambdas,
    gain_a,
    gain_b,
    out_a,
    out_b,
    residual,
    norm_gain,
    route_ids,
    route_weights,
    w_gate,
    w_up,
    w_down,
):
    core = lax.axis_index("c").astype(jnp.int32)
    gate_up, *downs = expert_weights(w_gate, w_up, w_down, core)
    target = slots_of(route_ids)
    rows_here, _ = route_ids.shape
    model_width = residual.shape[1]
    sends = 2 * N4 * N4
    slots = jnp.arange(2 * sends, dtype=jnp.int32)
    layout = jnp.any(target[None, :, :] == slots[:, None, None], axis=2).astype(bf16)
    shares = jnp.where(target[:, :, None] == slots, route_weights[:, :, None], 0.0).sum(axis=1)
    coarse = shares.astype(bf16).astype(f32)
    shares = jnp.concatenate([coarse, shares - coarse], axis=0).astype(bf16)
    projected = attention(
        query_a,
        key_a,
        value_a,
        query_b,
        key_b,
        value_b,
        lambdas,
        gain_a,
        gain_b,
        out_a,
        out_b,
        (layout, shares),
    )
    mixed = (residual.astype(f32) + projected).astype(bf16)
    widened = mixed.astype(f32)
    normed = (
        widened
        * lax.rsqrt(jnp.mean(widened * widened, axis=1, keepdims=True) + EPSILON)
        * norm_gain
    ).astype(bf16)
    leaving = jnp.dot(layout, normed, preferred_element_type=f32).astype(bf16)
    leaving = leaving.reshape(sends, 2, model_width)
    arrived = lax.all_to_all(leaving, ("y", "x", "c"), split_axis=0, concat_axis=0, tiled=True)
    arrived = arrived.reshape(2 * sends, HALVES, model_width // HALVES)
    summed = experts(jnp.swapaxes(arrived, 0, 1), gate_up, downs)
    summed = summed.reshape(sends, 2, model_width)
    returned = lax.all_to_all(summed, ("y", "x", "c"), split_axis=0, concat_axis=0, tiled=True)
    results = returned.reshape(2 * sends, model_width)
    combined = jnp.dot(shares, results, preferred_element_type=f32)
    combined = combined[:rows_here] + combined[rows_here:]
    return (widened + combined).astype(bf16)


def solution(mesh):
    split = Mesh(mesh.devices.reshape(N4, N4, NZ, 2), ALL)
    placed = (
        P(SP, TP, None),
        P(SP, TP, None),
        P(SP, TP, None),
        P(SP, TP, None),
        P(SP, TP, None),
        P(SP, TP, None),
        P(None, TP),
        P(),
        P(),
        P(TP, None),
        P(TP, None),
        P(ALL, None),
        P(),
        P(ALL, None),
        P(ALL, None),
        P(SP, None, TP),
        P(SP, None, TP),
        P(SP, TP, None),
    )

    return jax.shard_map(
        per_device, mesh=split, in_specs=placed, out_specs=P(ALL, None), check_vma=False
    )
```

```python
import functools

import jax
import jax.numpy as jnp
from jax import lax
from jax.experimental import pallas as pl
from jax.experimental.pallas import tpu as pltpu
from jax.sharding import Mesh
from jax.sharding import PartitionSpec as P


TP = ("z", "c")
SP = ("y", "x")
ALL = ("y", "x", "z", "c")

EPSILON = 1e-06
LIMIT = 7.0
SLOPE = 1.702
LOG2E = 1.4426950408889634

N4 = 4
NZ = 8
TOK = 256
CHUNK = 128
STAT = 16
DA = 128
DB = 64
VA = 256
VB = 128
f32 = jnp.float32
bf16 = jnp.bfloat16


def shifted(array, axis, count, by):
    return lax.ppermute(array, axis, [(i, (i + by) % count) for i in range(count)])


def one_group(q_ref, q_at, sources, k_at, out, half, width, value_width):
    rows = [
        q_ref[pl.ds(pl.multiple_of(z * 32 + half * 16, 16), 16), q_at : q_at + 2 * width]
        for z in range(NZ)
    ]
    q = jnp.concatenate(rows, axis=0)
    here = pl.ds(pl.multiple_of(half * CHUNK, CHUNK), CHUNK)
    scaling = width ** (-0.5) * LOG2E
    lane = lax.broadcasted_iota(jnp.int32, (CHUNK, 128), 1)
    stats = jnp.zeros((CHUNK, 128), f32)
    v_at = k_at + 2 * width
    for which in range(2):
        if width < 128:
            mine = lax.broadcasted_iota(jnp.int32, q.shape, 1) // width == which
            part = jnp.where(mine, q, jnp.zeros_like(q))
            keys = slice(k_at, k_at + 2 * width)
        else:
            part = q[:, which * width : (which + 1) * width]
            keys = slice(k_at + which * width, k_at + (which + 1) * width)
        scores = [
            lax.dot_general(
                part, ref[:, keys], (((1,), (1,)), ((), ())), preferred_element_type=f32
            )
            for ref in sources
        ]
        scores = jnp.concatenate(scores, axis=1) * scaling
        highest = jnp.max(scores, axis=1, keepdims=True).astype(bf16).astype(f32)
        expo = jnp.exp2(scores - highest)
        total = jnp.sum(expo, axis=1, keepdims=True)
        expo = expo.astype(bf16)
        carried = sum(
            jnp.dot(
                expo[:, i * TOK : (i + 1) * TOK],
                ref[:, v_at : v_at + value_width],
                preferred_element_type=f32,
            )
            for i, ref in enumerate(sources)
        )
        out[here, which * value_width : (which + 1) * value_width] = carried.astype(bf16)
        coarse = total.astype(bf16).astype(f32)
        for at, stat in enumerate((highest, coarse, total - coarse)):
            stats = jnp.where(lane == 3 * which + at, stat, stats)
    out[TOK : TOK + STAT, here] = stats.T[:STAT, :].astype(bf16)


def partial_kernel(*refs):
    xs, ys, (q_a, q_b, out_a, out_b) = refs[:4], refs[4:8], refs[8:]
    out_a[TOK:, :] = jnp.zeros((STAT, 2 * VA), bf16)

    def step(half, carry):
        one_group(q_a, 2 * DB + VB, xs, 0, out_a, half, DA, VA)
        one_group(q_b, 2 * DA + VA, ys, 0, out_b, half, DB, VB)
        return carry

    lax.fori_loop(0, 2, step, 0)


def partial_attention(xs, ys, block):
    vmem = pl.BlockSpec(memory_space=pltpu.VMEM)
    return pl.pallas_call(
        partial_kernel,
        out_shape=[
            jax.ShapeDtypeStruct((TOK + STAT, 2 * VA), bf16),
            jax.ShapeDtypeStruct((TOK + STAT, 2 * VB), bf16),
        ],
        in_specs=[vmem] * 10,
        out_specs=[vmem] * 2,
        cost_estimate=pl.CostEstimate(
            flops=1_500_000_000, bytes_accessed=3_000_000, transcendentals=1_048_576
        ),
        name="partial_attention",
    )(*xs, *ys, ys[block], xs[block])


def merge_group(parts, stat_scr, rows, value_width, weight, gain):
    lanes = stat_scr[rows, :]
    column = lambda part, at: lanes[:, STAT * part + at : STAT * part + at + 1]
    heard = []
    for which in range(2):
        maxima = [column(i, 3 * which) for i in range(4)]
        highest = jnp.maximum(jnp.maximum(maxima[0], maxima[1]), jnp.maximum(maxima[2], maxima[3]))
        total, summed = 0.0, 0.0
        for i in range(4):
            factor = jnp.exp2(maxima[i] - highest)
            total = total + factor * (column(i, 3 * which + 1) + column(i, 3 * which + 2))
            values = parts[i][rows, which * value_width : (which + 1) * value_width]
            summed = summed + factor * values.astype(f32)
        heard.append(summed / total)
    differ = heard[0] - weight * heard[1]
    scaled = lax.rsqrt(jnp.mean(differ * differ, axis=1, keepdims=True) + EPSILON)
    return (differ * scaled * gain).astype(bf16)


def merge_kernel(core, lam, gain_a, gain_b, *refs):
    pa, pb = refs[:4], refs[4:8]
    away, mine, sa, sb, att = refs[-5:]
    for parts, scr in ((pa, sa), (pb, sb)):
        rows = [p[TOK:, :TOK].astype(f32) for p in parts]
        rows.append(jnp.zeros((128 - 4 * STAT, TOK), f32))
        scr[...] = jnp.concatenate(rows, axis=0).T

    def step(n, carry):
        rows = pl.ds(pl.multiple_of(n * 64, 64), 64)
        att[rows, :VA] = merge_group(pa, sa, rows, VA, lam[0], gain_a[...])
        att[rows, VA:] = merge_group(pb, sb, rows, VB, lam[1], gain_b[...])
        return carry

    lax.fori_loop(0, TOK // 64, step, 0)
    half = TOK // 2
    me = core[0]
    away[...] = att[pl.ds(pl.multiple_of((1 - me) * half, half), half), :]
    mine[...] = att[pl.ds(pl.multiple_of(me * half, half), half), :]


def merged(parts_a, parts_b, lam, gain_a, gain_b, core, first):
    smem = pl.BlockSpec(memory_space=pltpu.SMEM)
    vmem = pl.BlockSpec(memory_space=pltpu.VMEM)
    out = jax.ShapeDtypeStruct((TOK // 2, VA + VB), bf16)
    return pl.pallas_call(
        merge_kernel,
        out_shape=[out, out],
        in_specs=[smem, smem] + [vmem] * 10 + [pl.BlockSpec(memory_space=pl.ANY)] * len(first),
        out_specs=[vmem, vmem],
        scratch_shapes=[
            pltpu.VMEM((TOK, 128), f32),
            pltpu.VMEM((TOK, 128), f32),
            pltpu.VMEM((TOK, VA + VB), bf16),
        ],
        cost_estimate=pl.CostEstimate(
            flops=800_000_000, bytes_accessed=2_000_000, transcendentals=20_000
        ),
        name="merge_parts",
    )(
        core.reshape(1),
        lam,
        gain_a.reshape(1, -1),
        gain_b.reshape(1, -1),
        *parts_a,
        *parts_b,
        *first,
    )


def project_kernel(mine, joined, wa, wb, xa, xb, out):
    total = jnp.dot(mine[:, :VA], wa[...], preferred_element_type=f32)
    total += jnp.dot(joined[:, :VA], xa[...], preferred_element_type=f32)
    total += jnp.dot(mine[:, VA:], wb[...], preferred_element_type=f32)
    total += jnp.dot(joined[:, VA:], xb[...], preferred_element_type=f32)
    out[...] = total


def project(mine, joined, wa, wb, xa, xb):
    width, tile = wa.shape[1], 1024
    whole = pl.BlockSpec(mine.shape, lambda i: (0, 0))
    deep = pl.BlockSpec((VA, tile), lambda i: (0, i))
    flat = pl.BlockSpec((VB, tile), lambda i: (0, i))
    return pl.pallas_call(
        project_kernel,
        grid=(width // tile,),
        out_shape=jax.ShapeDtypeStruct((mine.shape[0], width), f32),
        in_specs=[whole, whole, deep, flat, deep, flat],
        out_specs=pl.BlockSpec((mine.shape[0], tile), lambda i: (0, i)),
        cost_estimate=pl.CostEstimate(
            flops=3_000_000_000, bytes_accessed=8_000_000, transcendentals=0
        ),
        name="project",
    )(mine, joined, wa, wb, xa, xb)


def sum_over_z(own):
    z = lax.axis_index("z")
    pick = lambda k: lax.dynamic_index_in_dim(own, (z + k + NZ) % NZ, 0, keepdims=False)
    half = own.shape[2] // 2
    third, fourth, arrived = {}, {}, {}
    for sign in (1, -1):
        part = pick(4)[:, :half] if sign == 1 else pick(4)[:, half:]
        fourth[sign] = shifted(part.astype(bf16), "z", NZ, 2 * sign)
        third[sign] = shifted(pick(3 * sign).astype(bf16), "z", NZ, sign)
    for sign in (1, -1):
        padding = ((0, 0), (0, half)) if sign == 1 else ((0, 0), (half, 0))
        part = pick(2 * sign) + third[sign].astype(f32)
        part = part + jnp.pad(fourth[sign].astype(f32), padding)
        arrived[sign] = shifted(part.astype(bf16), "z", NZ, sign)
    for sign in (1, -1):
        part = pick(sign) + arrived[sign].astype(f32)
        arrived[sign] = shifted(part.astype(bf16), "z", NZ, sign)
    return pick(0) + arrived[1].astype(f32) + arrived[-1].astype(f32)


def attention(query_a, key_a, value_a, query_b, key_b, value_b, lambdas, gain_a, gain_b, out_a, out_b, first):
    flat = lambda a: a.reshape(TOK, -1)
    for_x = jnp.concatenate([flat(key_a), flat(value_a), flat(query_b)], axis=1)
    for_y = jnp.concatenate([flat(key_b), flat(value_b), flat(query_a)], axis=1)
    order = (2, 1, 3)
    got_x = {k: shifted(for_x, "x", N4, k) for k in order}
    got_y = {k: shifted(for_y, "y", N4, k) for k in order}
    xs = [for_x] + [got_x[k] for k in (1, 2, 3)]
    ys = [for_y] + [got_y[k] for k in (1, 2, 3)]
    parts, back = {}, {}
    for k in (*order, 0):
        parts[k] = partial_attention(xs, ys, k)
        if k:
            back[k] = shifted(parts[k][0], "y", N4, -k), shifted(parts[k][1], "x", N4, -k)
    parts_a = [parts[0][0]] + [back[k][0] for k in (1, 2, 3)]
    parts_b = [parts[0][1]] + [back[k][1] for k in (1, 2, 3)]
    core = lax.axis_index("c").astype(jnp.int32)
    away, mine = merged(parts_a, parts_b, lambdas.reshape(-1), gain_a, gain_b, core, first)
    other_a, other_b = shifted(out_a, "c", 2, 1), shifted(out_b, "c", 2, 1)
    own = project(mine, shifted(away, "c", 2, 1), out_a, out_b, other_a, other_b)
    return sum_over_z(own.reshape(NZ, 16, -1))


HALVES = 2
STEP = 1024


def gate_kernel(count, *refs):
    outs, (tokens, sums) = refs[-2 - count : -2], refs[-2:]
    pieces, weights = refs[: -3 - count], refs[-3 - count]
    rows = outs[0].shape[0]
    for at, half in enumerate(pieces):
        row, column = at // HALVES * rows, at % HALVES * half.shape[1]
        tokens[row : row + rows, column : column + half.shape[1]] = half[...]
    sums[...] = jnp.zeros_like(sums)

    def step(n, carry):
        part = pl.ds(pl.multiple_of(n * STEP, STEP), STEP)
        sums[...] += jnp.dot(tokens[:, part], weights[part, :], preferred_element_type=f32)
        return carry

    lax.fori_loop(0, weights.shape[0] // STEP, step, 0)
    units = outs[0].shape[1]
    for at, out in enumerate(outs):
        here = slice(at * rows, (at + 1) * rows)
        gate = jnp.minimum(sums[here, :units], LIMIT)
        upward = jnp.clip(sums[here, units:], -LIMIT, LIMIT) + 1.0
        out[...] = (gate * jax.nn.sigmoid(SLOPE * gate) * upward).astype(bf16)


def gated_units(blocks, weights):
    vmem = pl.BlockSpec(memory_space=pltpu.VMEM)
    pieces = [piece for block in blocks for piece in block]
    count, rows = len(blocks), pieces[0].shape[0]
    depth, both = weights.shape
    return pl.pallas_call(
        functools.partial(gate_kernel, count),
        out_shape=[jax.ShapeDtypeStruct((rows, both // 2), bf16)] * count,
        in_specs=[vmem] * (len(pieces) + 1),
        out_specs=[vmem] * count,
        scratch_shapes=[
            pltpu.VMEM((count * rows, depth), bf16),
            pltpu.VMEM((count * rows, both), f32),
        ],
        cost_estimate=pl.CostEstimate(
            flops=4_000_000_000, bytes_accessed=6_000_000, transcendentals=count * rows * 256
        ),
    )(*pieces, weights)


def experts(block, gate_up, downs):
    width = block.shape[1] // HALVES
    ring = {(0, h): block[:, h * width : (h + 1) * width] for h in range(HALVES)}
    for k in range(1, 5):
        for h in range(HALVES):
            if k < 4 or h == 0:
                ring[k, h] = shifted(ring[k - 1, h], "z", NZ, 1)
            if k < 4 or h == 1:
                ring[-k, h] = shifted(ring[1 - k, h], "z", NZ, -1)
    ring[4, 1] = ring[-4, 1]
    units = {}
    for offsets in ((0, 1, -1, 2, -2), (3, -3), (4,)):
        outs = gated_units([[ring[k, h] for h in range(HALVES)] for k in offsets], gate_up)
        for k, out in zip(offsets, outs):
            units[-k] = out
    units[4] = units[-4]

    def share(offset, h):
        return jnp.dot(units[offset], downs[h], preferred_element_type=f32)

    carried = {}
    for k in range(4, 0, -1):
        for h in range(HALVES):
            for sign, start in ((-1, 4 - h), (1, 3 + h)):
                if k > start:
                    continue
                part = share(sign * k, h)
                if k < start:
                    part = part + carried[sign, h].astype(f32)
                carried[sign, h] = shifted(part.astype(bf16), "z", NZ, sign)
    total = []
    for h in range(HALVES):
        part = share(0, h) + carried[-1, h].astype(f32) + carried[1, h].astype(f32)
        total.append(part.astype(bf16))
    return jnp.concatenate(total, axis=1)


def pack_kernel(core, gate, gate_other, upward, upward_other, *refs):
    downs, (both, *lowers) = refs[:4], refs[4:]
    units = gate.shape[2]
    for at, ref in enumerate((gate, gate_other, upward, upward_other)):
        both[:, at * units : (at + 1) * units] = ref[0]
    for h, lower in enumerate(lowers):
        for at in range(2):
            lower[at * units : (at + 1) * units, :] = downs[2 * h + at][0]


def expert_weights(w_gate, w_up, w_down, core):
    _, depth, units = w_gate.shape
    tile = 512
    deep = pl.BlockSpec((1, tile, units), lambda i, c: (c[0], i, 0))
    steps = depth // tile
    thin = tile // HALVES
    flat = [
        pl.BlockSpec((1, units, thin), lambda i, c, h=h: (c[0], 0, i + h * steps))
        for h in range(HALVES)
    ]

    def other(w):
        return shifted(w, "c", 2, 1)

    return pl.pallas_call(
        pack_kernel,
        grid_spec=pltpu.PrefetchScalarGridSpec(
            num_scalar_prefetch=1,
            grid=(depth // tile,),
            in_specs=[deep] * 4 + [flat[0]] * 2 + [flat[1]] * 2,
            out_specs=[
                pl.BlockSpec((tile, 4 * units), lambda i, c: (i, 0)),
                *[pl.BlockSpec((2 * units, thin), lambda i, c: (0, i))] * HALVES,
            ],
        ),
        out_shape=[
            jax.ShapeDtypeStruct((depth, 4 * units), bf16),
            *[jax.ShapeDtypeStruct((2 * units, depth // HALVES), bf16)] * HALVES,
        ],
        cost_estimate=pl.CostEstimate(
            flops=3_000_000_000, bytes_accessed=12_000_000, transcendentals=0
        ),
        name="pack_weights",
    )(core.reshape(1), w_gate, other(w_gate), w_up, other(w_up), *[w_down, other(w_down)] * HALVES)


def slots_of(ids):
    flat = ids.reshape(-1)
    same = (flat[:, None] == flat[None, :]).astype(jnp.int32)
    place = jnp.sum(same * jnp.tril(jnp.ones_like(same), -1), axis=1)
    return (flat * 2 + place).reshape(ids.shape)


def per_device(
    query_a,
    key_a,
    value_a,
    query_b,
    key_b,
    value_b,
    lambdas,
    gain_a,
    gain_b,
    out_a,
    out_b,
    residual,
    norm_gain,
    route_ids,
    route_weights,
    w_gate,
    w_up,
    w_down,
):
    core = lax.axis_index("c").astype(jnp.int32)
    gate_up, *downs = expert_weights(w_gate, w_up, w_down, core)
    target = slots_of(route_ids)
    rows_here, _ = route_ids.shape
    model_width = residual.shape[1]
    sends = 2 * N4 * N4
    slots = jnp.arange(2 * sends, dtype=jnp.int32)
    layout = jnp.any(target[None, :, :] == slots[:, None, None], axis=2).astype(bf16)
    shares = jnp.where(target[:, :, None] == slots, route_weights[:, :, None], 0.0).sum(axis=1)
    coarse = shares.astype(bf16).astype(f32)
    shares = jnp.concatenate([coarse, shares - coarse], axis=0).astype(bf16)
    projected = attention(
        query_a,
        key_a,
        value_a,
        query_b,
        key_b,
        value_b,
        lambdas,
        gain_a,
        gain_b,
        out_a,
        out_b,
        (layout, shares),
    )
    mixed = (residual.astype(f32) + projected).astype(bf16)
    widened = mixed.astype(f32)
    normed = (
        widened
        * lax.rsqrt(jnp.mean(widened * widened, axis=1, keepdims=True) + EPSILON)
        * norm_gain
    ).astype(bf16)
    leaving = jnp.dot(layout, normed, preferred_element_type=f32).astype(bf16)
    leaving = leaving.reshape(sends, 2, model_width)
    arrived = lax.all_to_all(leaving, ("y", "x", "c"), split_axis=0, concat_axis=0, tiled=True)
    summed = experts(arrived.reshape(2 * sends, model_width), gate_up, downs)
    summed = summed.reshape(sends, 2, model_width)
    returned = lax.all_to_all(summed, ("y", "x", "c"), split_axis=0, concat_axis=0, tiled=True)
    results = returned.reshape(2 * sends, model_width)
    combined = jnp.dot(shares, results, preferred_element_type=f32)
    combined = combined[:rows_here] + combined[rows_here:]
    return (widened + combined).astype(bf16)


def solution(mesh):
    split = Mesh(mesh.devices.reshape(N4, N4, NZ, 2), ALL)
    placed = (
        P(SP, TP, None),
        P(SP, TP, None),
        P(SP, TP, None),
        P(SP, TP, None),
        P(SP, TP, None),
        P(SP, TP, None),
        P(None, TP),
        P(),
        P(),
        P(TP, None),
        P(TP, None),
        P(ALL, None),
        P(),
        P(ALL, None),
        P(ALL, None),
        P(SP, None, TP),
        P(SP, None, TP),
        P(SP, TP, None),
    )

    return jax.shard_map(
        per_device, mesh=split, in_specs=placed, out_specs=P(ALL, None), check_vma=False
    )
```

```python
import functools

import jax
import jax.numpy as jnp
from jax import lax
from jax.experimental import pallas as pl
from jax.experimental.pallas import tpu as pltpu
from jax.sharding import Mesh
from jax.sharding import PartitionSpec as P


TP = ("z", "c")
SP = ("y", "x")
ALL = ("y", "x", "z", "c")

EPSILON = 1e-06
LIMIT = 7.0
SLOPE = 1.702
LOG2E = 1.4426950408889634

N4 = 4
NZ = 8
TOK = 256
CHUNK = TOK
STAT = 16
DA = 128
DB = 64
VA = 256
VB = 128
f32 = jnp.float32
bf16 = jnp.bfloat16


def shifted(array, axis, count, by):
    return lax.ppermute(array, axis, [(i, (i + by) % count) for i in range(count)])


def one_group(q_ref, q_at, sources, k_at, out, width, value_width):
    rows = [
        q_ref[z * 32 + half * 16 : z * 32 + half * 16 + 16, q_at : q_at + 2 * width]
        for half in range(2)
        for z in range(NZ)
    ]
    q = jnp.concatenate(rows, axis=0)
    here = slice(0, CHUNK)
    scaling = width ** (-0.5) * LOG2E
    lane = lax.broadcasted_iota(jnp.int32, (CHUNK, 128), 1)
    stats = jnp.zeros((CHUNK, 128), f32)
    v_at = k_at + 2 * width
    for which in range(2):
        if width < 128:
            mine = lax.broadcasted_iota(jnp.int32, q.shape, 1) // width == which
            part = jnp.where(mine, q, jnp.zeros_like(q))
            keys = slice(k_at, k_at + 2 * width)
        else:
            part = q[:, which * width : (which + 1) * width]
            keys = slice(k_at + which * width, k_at + (which + 1) * width)
        scores = [
            lax.dot_general(
                part, ref[:, keys], (((1,), (1,)), ((), ())), preferred_element_type=f32
            )
            for ref in sources
        ]
        scores = jnp.concatenate(scores, axis=1) * scaling
        highest = jnp.max(scores, axis=1, keepdims=True).astype(bf16).astype(f32)
        expo = jnp.exp2(scores - highest)
        total = jnp.sum(expo, axis=1, keepdims=True)
        expo = expo.astype(bf16)
        carried = sum(
            jnp.dot(
                expo[:, i * TOK : (i + 1) * TOK],
                ref[:, v_at : v_at + value_width],
                preferred_element_type=f32,
            )
            for i, ref in enumerate(sources)
        )
        out[here, which * value_width : (which + 1) * value_width] = carried.astype(bf16)
        coarse = total.astype(bf16).astype(f32)
        for at, stat in enumerate((highest, coarse, total - coarse)):
            stats = jnp.where(lane == 3 * which + at, stat, stats)
    out[TOK : TOK + STAT, here] = stats.T[:STAT, :].astype(bf16)


def partial_kernel(*refs):
    xs, ys, (q_a, q_b, out_a, out_b) = refs[:4], refs[4:8], refs[8:]
    out_a[TOK:, :] = jnp.zeros((STAT, 2 * VA), bf16)

    one_group(q_a, 2 * DB + VB, xs, 0, out_a, DA, VA)
    one_group(q_b, 2 * DA + VA, ys, 0, out_b, DB, VB)


def partial_attention(xs, ys, block):
    vmem = pl.BlockSpec(memory_space=pltpu.VMEM)
    return pl.pallas_call(
        partial_kernel,
        out_shape=[
            jax.ShapeDtypeStruct((TOK + STAT, 2 * VA), bf16),
            jax.ShapeDtypeStruct((TOK + STAT, 2 * VB), bf16),
        ],
        in_specs=[vmem] * 10,
        out_specs=[vmem] * 2,
        cost_estimate=pl.CostEstimate(
            flops=1_500_000_000, bytes_accessed=3_000_000, transcendentals=1_048_576
        ),
        name="partial_attention",
    )(*xs, *ys, ys[block], xs[block])


def merge_group(parts, stat_scr, rows, value_width, weight, gain):
    lanes = stat_scr[rows, :]
    column = lambda part, at: lanes[:, STAT * part + at : STAT * part + at + 1]
    heard = []
    for which in range(2):
        maxima = [column(i, 3 * which) for i in range(4)]
        highest = jnp.maximum(jnp.maximum(maxima[0], maxima[1]), jnp.maximum(maxima[2], maxima[3]))
        total, summed = 0.0, 0.0
        for i in range(4):
            factor = jnp.exp2(maxima[i] - highest)
            total = total + factor * (column(i, 3 * which + 1) + column(i, 3 * which + 2))
            values = parts[i][rows, which * value_width : (which + 1) * value_width]
            summed = summed + factor * values.astype(f32)
        heard.append(summed / total)
    differ = heard[0] - weight * heard[1]
    scaled = lax.rsqrt(jnp.mean(differ * differ, axis=1, keepdims=True) + EPSILON)
    return (differ * scaled * gain).astype(bf16)


def merge_kernel(core, lam, gain_a, gain_b, *refs):
    pa, pb = refs[:4], refs[4:8]
    away, mine, sa, sb, att = refs[-5:]
    for parts, scr in ((pa, sa), (pb, sb)):
        rows = [p[TOK:, :TOK].astype(f32) for p in parts]
        rows.append(jnp.zeros((128 - 4 * STAT, TOK), f32))
        scr[...] = jnp.concatenate(rows, axis=0).T

    def step(n, carry):
        rows = pl.ds(pl.multiple_of(n * 64, 64), 64)
        att[rows, :VA] = merge_group(pa, sa, rows, VA, lam[0], gain_a[...])
        att[rows, VA:] = merge_group(pb, sb, rows, VB, lam[1], gain_b[...])
        return carry

    lax.fori_loop(0, TOK // 64, step, 0)
    half = TOK // 2
    me = core[0]
    away[...] = att[pl.ds(pl.multiple_of((1 - me) * half, half), half), :]
    mine[...] = att[pl.ds(pl.multiple_of(me * half, half), half), :]


def merged(parts_a, parts_b, lam, gain_a, gain_b, core, first):
    smem = pl.BlockSpec(memory_space=pltpu.SMEM)
    vmem = pl.BlockSpec(memory_space=pltpu.VMEM)
    out = jax.ShapeDtypeStruct((TOK // 2, VA + VB), bf16)
    return pl.pallas_call(
        merge_kernel,
        out_shape=[out, out],
        in_specs=[smem, smem] + [vmem] * 10 + [pl.BlockSpec(memory_space=pl.ANY)] * len(first),
        out_specs=[vmem, vmem],
        scratch_shapes=[
            pltpu.VMEM((TOK, 128), f32),
            pltpu.VMEM((TOK, 128), f32),
            pltpu.VMEM((TOK, VA + VB), bf16),
        ],
        cost_estimate=pl.CostEstimate(
            flops=800_000_000, bytes_accessed=2_000_000, transcendentals=20_000
        ),
        name="merge_parts",
    )(
        core.reshape(1),
        lam,
        gain_a.reshape(1, -1),
        gain_b.reshape(1, -1),
        *parts_a,
        *parts_b,
        *first,
    )


def project_kernel(mine, joined, wa, wb, xa, xb, out):
    total = jnp.dot(mine[:, :VA], wa[...], preferred_element_type=f32)
    total += jnp.dot(joined[:, :VA], xa[...], preferred_element_type=f32)
    total += jnp.dot(mine[:, VA:], wb[...], preferred_element_type=f32)
    total += jnp.dot(joined[:, VA:], xb[...], preferred_element_type=f32)
    out[...] = total


def project(mine, joined, wa, wb, xa, xb):
    width, tile = wa.shape[1], 1024
    whole = pl.BlockSpec(mine.shape, lambda i: (0, 0))
    deep = pl.BlockSpec((VA, tile), lambda i: (0, i))
    flat = pl.BlockSpec((VB, tile), lambda i: (0, i))
    return pl.pallas_call(
        project_kernel,
        grid=(width // tile,),
        out_shape=jax.ShapeDtypeStruct((mine.shape[0], width), f32),
        in_specs=[whole, whole, deep, flat, deep, flat],
        out_specs=pl.BlockSpec((mine.shape[0], tile), lambda i: (0, i)),
        cost_estimate=pl.CostEstimate(
            flops=3_000_000_000, bytes_accessed=8_000_000, transcendentals=0
        ),
        name="project",
    )(mine, joined, wa, wb, xa, xb)


def sum_over_z(own):
    z = lax.axis_index("z")
    pick = lambda k: lax.dynamic_index_in_dim(own, (z + k + NZ) % NZ, 0, keepdims=False)
    half = own.shape[2] // 2
    third, fourth, arrived = {}, {}, {}
    for sign in (1, -1):
        part = pick(4)[:, :half] if sign == 1 else pick(4)[:, half:]
        fourth[sign] = shifted(part.astype(bf16), "z", NZ, 2 * sign)
        third[sign] = shifted(pick(3 * sign).astype(bf16), "z", NZ, sign)
    for sign in (1, -1):
        padding = ((0, 0), (0, half)) if sign == 1 else ((0, 0), (half, 0))
        part = pick(2 * sign) + third[sign].astype(f32)
        part = part + jnp.pad(fourth[sign].astype(f32), padding)
        arrived[sign] = shifted(part.astype(bf16), "z", NZ, sign)
    for sign in (1, -1):
        part = pick(sign) + arrived[sign].astype(f32)
        arrived[sign] = shifted(part.astype(bf16), "z", NZ, sign)
    return pick(0) + arrived[1].astype(f32) + arrived[-1].astype(f32)


def attention(query_a, key_a, value_a, query_b, key_b, value_b, lambdas, gain_a, gain_b, out_a, out_b, first):
    flat = lambda a: a.reshape(TOK, -1)
    for_x = jnp.concatenate([flat(key_a), flat(value_a), flat(query_b)], axis=1)
    for_y = jnp.concatenate([flat(key_b), flat(value_b), flat(query_a)], axis=1)
    order = (2, 1, 3)
    got_x, got_y = {}, {}
    for k in order:
        got_x[k] = shifted(for_x, "x", N4, k)
        got_y[k] = shifted(for_y, "y", N4, k)
    xs = [for_x] + [got_x[k] for k in (1, 2, 3)]
    ys = [for_y] + [got_y[k] for k in (1, 2, 3)]
    parts, back = {}, {}
    for k in (*order, 0):
        parts[k] = partial_attention(xs, ys, k)
        if k:
            back[k] = shifted(parts[k][0], "y", N4, -k), shifted(parts[k][1], "x", N4, -k)
    parts_a = [parts[0][0]] + [back[k][0] for k in (1, 2, 3)]
    parts_b = [parts[0][1]] + [back[k][1] for k in (1, 2, 3)]
    core = lax.axis_index("c").astype(jnp.int32)
    away, mine = merged(parts_a, parts_b, lambdas.reshape(-1), gain_a, gain_b, core, first)
    other_a, other_b = shifted(out_a, "c", 2, 1), shifted(out_b, "c", 2, 1)
    own = project(mine, shifted(away, "c", 2, 1), out_a, out_b, other_a, other_b)
    return sum_over_z(own.reshape(NZ, 16, -1))


HALVES = 2
STEP = 1024


def gate_kernel(count, *refs):
    outs, (tokens, sums) = refs[-2 - count : -2], refs[-2:]
    pieces, weights = refs[: -3 - count], refs[-3 - count]
    rows = outs[0].shape[0]
    for at, half in enumerate(pieces):
        row, column = at // HALVES * rows, at % HALVES * half.shape[1]
        tokens[row : row + rows, column : column + half.shape[1]] = half[...]
    sums[...] = jnp.zeros_like(sums)

    def step(n, carry):
        part = pl.ds(pl.multiple_of(n * STEP, STEP), STEP)
        sums[...] += jnp.dot(tokens[:, part], weights[part, :], preferred_element_type=f32)
        return carry

    lax.fori_loop(0, weights.shape[0] // STEP, step, 0)
    units = outs[0].shape[1]
    for at, out in enumerate(outs):
        here = slice(at * rows, (at + 1) * rows)
        gate = jnp.minimum(sums[here, :units], LIMIT)
        upward = jnp.clip(sums[here, units:], -LIMIT, LIMIT) + 1.0
        out[...] = (gate * jax.nn.sigmoid(SLOPE * gate) * upward).astype(bf16)


def gated_units(blocks, weights):
    vmem = pl.BlockSpec(memory_space=pltpu.VMEM)
    pieces = [piece for block in blocks for piece in block]
    count, rows = len(blocks), pieces[0].shape[0]
    depth, both = weights.shape
    return pl.pallas_call(
        functools.partial(gate_kernel, count),
        out_shape=[jax.ShapeDtypeStruct((rows, both // 2), bf16)] * count,
        in_specs=[vmem] * (len(pieces) + 1),
        out_specs=[vmem] * count,
        scratch_shapes=[
            pltpu.VMEM((count * rows, depth), bf16),
            pltpu.VMEM((count * rows, both), f32),
        ],
        cost_estimate=pl.CostEstimate(
            flops=4_000_000_000, bytes_accessed=6_000_000, transcendentals=count * rows * 256
        ),
    )(*pieces, weights)


def experts(block, gate_up, downs):
    width = block.shape[1] // HALVES
    ring = {(0, h): block[:, h * width : (h + 1) * width] for h in range(HALVES)}
    for k in range(1, 5):
        for h in range(HALVES):
            if k < 4 or h == 0:
                ring[k, h] = shifted(ring[k - 1, h], "z", NZ, 1)
            if k < 4 or h == 1:
                ring[-k, h] = shifted(ring[1 - k, h], "z", NZ, -1)
    ring[4, 1] = ring[-4, 1]
    units = {}
    for offsets in ((0, 1, -1, 2, -2), (3, -3), (4,)):
        outs = gated_units([[ring[k, h] for h in range(HALVES)] for k in offsets], gate_up)
        for k, out in zip(offsets, outs):
            units[-k] = out
    units[4] = units[-4]

    def share(offset, h):
        return jnp.dot(units[offset], downs[h], preferred_element_type=f32)

    carried = {}
    for k in range(4, 0, -1):
        for h in range(HALVES):
            for sign, start in ((-1, 4 - h), (1, 3 + h)):
                if k > start:
                    continue
                part = share(sign * k, h)
                if k < start:
                    part = part + carried[sign, h].astype(f32)
                carried[sign, h] = shifted(part.astype(bf16), "z", NZ, sign)
    total = []
    for h in range(HALVES):
        part = share(0, h) + carried[-1, h].astype(f32) + carried[1, h].astype(f32)
        total.append(part.astype(bf16))
    return jnp.concatenate(total, axis=1)


def pack_kernel(core, gate, gate_other, upward, upward_other, *refs):
    downs, (both, *lowers) = refs[:4], refs[4:]
    units = gate.shape[2]
    for at, ref in enumerate((gate, gate_other, upward, upward_other)):
        both[:, at * units : (at + 1) * units] = ref[0]
    for h, lower in enumerate(lowers):
        for at in range(2):
            lower[at * units : (at + 1) * units, :] = downs[2 * h + at][0]


def expert_weights(w_gate, w_up, w_down, core):
    _, depth, units = w_gate.shape
    tile = 512
    deep = pl.BlockSpec((1, tile, units), lambda i, c: (c[0], i, 0))
    steps = depth // tile
    thin = tile // HALVES
    flat = [
        pl.BlockSpec((1, units, thin), lambda i, c, h=h: (c[0], 0, i + h * steps))
        for h in range(HALVES)
    ]

    def other(w):
        return shifted(w, "c", 2, 1)

    return pl.pallas_call(
        pack_kernel,
        grid_spec=pltpu.PrefetchScalarGridSpec(
            num_scalar_prefetch=1,
            grid=(depth // tile,),
            in_specs=[deep] * 4 + [flat[0]] * 2 + [flat[1]] * 2,
            out_specs=[
                pl.BlockSpec((tile, 4 * units), lambda i, c: (i, 0)),
                *[pl.BlockSpec((2 * units, thin), lambda i, c: (0, i))] * HALVES,
            ],
        ),
        out_shape=[
            jax.ShapeDtypeStruct((depth, 4 * units), bf16),
            *[jax.ShapeDtypeStruct((2 * units, depth // HALVES), bf16)] * HALVES,
        ],
        cost_estimate=pl.CostEstimate(
            flops=3_000_000_000, bytes_accessed=12_000_000, transcendentals=0
        ),
        name="pack_weights",
    )(core.reshape(1), w_gate, other(w_gate), w_up, other(w_up), *[w_down, other(w_down)] * HALVES)


def slots_of(ids):
    flat = ids.reshape(-1)
    same = (flat[:, None] == flat[None, :]).astype(jnp.int32)
    place = jnp.sum(same * jnp.tril(jnp.ones_like(same), -1), axis=1)
    return (flat * 2 + place).reshape(ids.shape)


def per_device(
    query_a,
    key_a,
    value_a,
    query_b,
    key_b,
    value_b,
    lambdas,
    gain_a,
    gain_b,
    out_a,
    out_b,
    residual,
    norm_gain,
    route_ids,
    route_weights,
    w_gate,
    w_up,
    w_down,
):
    core = lax.axis_index("c").astype(jnp.int32)
    gate_up, *downs = expert_weights(w_gate, w_up, w_down, core)
    target = slots_of(route_ids)
    rows_here, _ = route_ids.shape
    model_width = residual.shape[1]
    sends = 2 * N4 * N4
    slots = jnp.arange(2 * sends, dtype=jnp.int32)
    layout = jnp.any(target[None, :, :] == slots[:, None, None], axis=2).astype(bf16)
    shares = jnp.where(target[:, :, None] == slots, route_weights[:, :, None], 0.0).sum(axis=1)
    coarse = shares.astype(bf16).astype(f32)
    shares = jnp.concatenate([coarse, shares - coarse], axis=0).astype(bf16)
    projected = attention(
        query_a,
        key_a,
        value_a,
        query_b,
        key_b,
        value_b,
        lambdas,
        gain_a,
        gain_b,
        out_a,
        out_b,
        (layout, shares),
    )
    mixed = (residual.astype(f32) + projected).astype(bf16)
    widened = mixed.astype(f32)
    normed = (
        widened
        * lax.rsqrt(jnp.mean(widened * widened, axis=1, keepdims=True) + EPSILON)
        * norm_gain
    ).astype(bf16)
    leaving = jnp.dot(layout, normed, preferred_element_type=f32).astype(bf16)
    leaving = leaving.reshape(sends, 2, model_width)
    arrived = lax.all_to_all(leaving, ("y", "x", "c"), split_axis=0, concat_axis=0, tiled=True)
    summed = experts(arrived.reshape(2 * sends, model_width), gate_up, downs)
    summed = summed.reshape(sends, 2, model_width)
    returned = lax.all_to_all(summed, ("y", "x", "c"), split_axis=0, concat_axis=0, tiled=True)
    results = returned.reshape(2 * sends, model_width)
    combined = jnp.dot(shares, results, preferred_element_type=f32)
    combined = combined[:rows_here] + combined[rows_here:]
    return (widened + combined).astype(bf16)


def solution(mesh):
    split = Mesh(mesh.devices.reshape(N4, N4, NZ, 2), ALL)
    placed = (
        P(SP, TP, None),
        P(SP, TP, None),
        P(SP, TP, None),
        P(SP, TP, None),
        P(SP, TP, None),
        P(SP, TP, None),
        P(None, TP),
        P(),
        P(),
        P(TP, None),
        P(TP, None),
        P(ALL, None),
        P(),
        P(ALL, None),
        P(ALL, None),
        P(SP, None, TP),
        P(SP, None, TP),
        P(SP, TP, None),
    )

    return jax.shard_map(
        per_device, mesh=split, in_specs=placed, out_specs=P(ALL, None), check_vma=False
    )
```
